32 devices in a mesh: sp: 4 (over z), fs: 4 (over y, x), tp: 2 (over core).
Axes of the slice: x: 2, y: 2, z: 4, core: 2. Of those that a mesh axis runs over, the one named last changes fastest.
Arguments:
- tokens: bfloat16 [4, 1024, 2048], P('fs', 'sp'), may hold values from -6 to 6
- norm_gain: float32 [2048], replicated, may hold values from 0.1 to 1.9
- pool_input: bfloat16 [2048, 2048], P(('sp', 'fs'), 'tp'), may hold values from -0.125 to 0.125
- query_weight: bfloat16 [2048, 2048], P(('sp', 'fs'), 'tp'), may hold values from -20 to 20
- key_weight: bfloat16 [2048, 2048], P(('sp', 'fs'), 'tp'), may hold values from -1 to 1
- value_weight: bfloat16 [2048, 2048], P(('sp', 'fs'), 'tp'), may hold values from -0.125 to 0.125
- pool_map: bfloat16 [8, 256, 256], P('tp'), may hold values from -0.375 to 0.375
- pool_scale: float32 [2048], P('tp'), may hold values from 0.1 to 1.9
- head_gain: float32 [256], replicated, may hold values from 0.1 to 1.9
- diff_lambda: float32 [8], replicated, may hold values from 0.3 to 0.8
- out_pool: bfloat16 [2048, 2048], P('tp', ('sp', 'fs')), may hold values from -0.09375 to 0.09375
- out_heads: bfloat16 [2048, 2048], P('tp', ('sp', 'fs')), may hold values from -0.09375 to 0.09375
Outputs:
- layer_out: bfloat16 [4, 1024, 2048], P('fs', 'sp', 'tp')
The draws below stay inside these ranges and needn't reach their ends.
All inputs are finite; a program needn't handle non-finite values.
Results may differ from the reference program's by a relative error of at most 0.018.
Values may be sent and summed in bfloat16 or wider, within the bound.
A program may use at most 64 MiB of HBM per device.

```python
import math
import jax
import jax.numpy as jnp
from jax import lax

D = 2048
HEADS = 8
HEAD_DIM = 128
POOL_GROUPS = 8
GROUP_DIM = 256
POOL_WIDTH = 2048
SEQ = 1024
SEQS = 4
N_TP = 2


def key_matrix(key):
    normal_part = jax.random.truncated_normal(jax.random.fold_in(key, 11), -6.0, 6.0, (D, 2 * HEADS * HEAD_DIM), jnp.float32)
    return normal_part * D ** (-0.5)


def draw_key_weight(key, part):
    return key_matrix(key).astype(jnp.bfloat16)


def draw_query_weight(key, part):
    normal_part = jax.random.truncated_normal(jax.random.fold_in(key, 12), -6.0, 6.0, (D, 2 * HEADS * HEAD_DIM), jnp.float32)
    result = normal_part * (3.0 / D) ** 0.5
    return result.astype(jnp.bfloat16)


def levels(key, shape, cuts, smallest, high):
    loudness, own = 1.0, jax.random.fold_in(key, 6)
    for dim, shards_of in cuts:
        draws = jnp.exp(jax.random.uniform(jax.random.fold_in(own, dim), (shards_of,), jnp.float32, smallest / len(cuts), high / len(cuts)))
        loudness = loudness * jnp.repeat(draws, shape[dim] // shards_of).reshape([-1 if axis == dim else 1 for axis in range(len(shape))])
    return loudness


def normal_values(key, extent, spread, limit, split=(), kind=jnp.bfloat16):
    array = jax.random.normal(key, extent, jnp.float32) * spread
    if len(split) > 0:
        array = levels(key, extent, split, -0.22, 0.18) * array
    return jnp.clip(array, min=-limit, max=limit).astype(kind)


def setup_inputs(seed: int = 0) -> dict:
    arg_keys = jax.random.split(jax.random.key(seed), 13)
    return {
        "tokens": normal_values(arg_keys[0], (SEQS, SEQ, D), 1.0, 6.0, ((0, 4), (1, 4))),
        "norm_gain": jnp.clip(1.0 + 0.18 * jax.random.normal(arg_keys[1], (D,), jnp.float32), 0.1, 1.9),
        "pool_input": normal_values(arg_keys[2], (D, POOL_WIDTH), D ** -0.5, 0.125, ((0, 16), (1, 2))),
        "query_weight": draw_query_weight(jax.random.fold_in(arg_keys[12], 71), 0),
        "key_weight": draw_key_weight(jax.random.fold_in(arg_keys[12], 71), 0),
        "value_weight": normal_values(arg_keys[5], (D, 2 * HEADS * HEAD_DIM), D ** -0.5, 0.125, ((0, 16), (1, 2))),
        "pool_map": normal_values(arg_keys[6], (POOL_GROUPS, GROUP_DIM, GROUP_DIM), GROUP_DIM ** -0.5, 0.375, ((0, 2),)),
        "pool_scale": jnp.clip(1.0 + 0.18 * jax.random.normal(arg_keys[7], (POOL_WIDTH,), jnp.float32), 0.1, 1.9),
        "head_gain": jnp.clip(1.0 + 0.18 * jax.random.normal(arg_keys[8], (2 * HEAD_DIM,), jnp.float32), 0.1, 1.9),
        "diff_lambda": jnp.clip(jax.random.uniform(arg_keys[9], (HEADS,), jnp.float32, 0.3, 0.8), 0.3, 0.8),
        "out_pool": normal_values(arg_keys[10], (POOL_WIDTH, D), (POOL_WIDTH + 2 * HEADS * HEAD_DIM) ** -0.5, 0.09375, ((0, 2), (1, 16))),
        "out_heads": normal_values(arg_keys[11], (2 * HEADS * HEAD_DIM, D), (POOL_WIDTH + 2 * HEADS * HEAD_DIM) ** -0.5, 0.09375, ((0, 2), (1, 16))),
    }


THETA = 500000.0
HEAD_SCALE = 0.8
NORM_EPS = 1e-06
HEAD_EPS = 1e-05

def rotate(tensor, positions):
    half = HEAD_DIM // 2
    freqs = 1.0 / THETA ** (jnp.arange(half, dtype=jnp.float32) * 2.0 / HEAD_DIM)
    angles = positions[:, None] * freqs[None, :]
    cosine = jnp.cos(angles)[:, None, None, :]
    sine = jnp.sin(angles)[:, None, None, :]
    floated = tensor.astype(jnp.float32)
    first = floated[..., :half]
    second = floated[..., half:]
    turned = jnp.concatenate([first * cosine - second * sine, second * cosine + first * sine], -1)
    return turned.astype(jnp.bfloat16)

def one_sequence(seq_tokens, norm_gain, pool_input, query_weight, key_weight, value_weight, pool_map, pool_scale, head_gain, diff_lambda, out_pool, out_heads):
    length = seq_tokens.shape[0]
    floated = seq_tokens.astype(jnp.float32)
    normed = (floated * lax.rsqrt(lax.optimization_barrier(jnp.mean(floated * floated, -1, keepdims=True)) + NORM_EPS) * norm_gain).astype(jnp.bfloat16)
    pool_in = jnp.dot(normed, pool_input, preferred_element_type=jnp.float32).astype(jnp.bfloat16)
    queries = jnp.dot(normed, query_weight, preferred_element_type=jnp.float32).astype(jnp.bfloat16)
    keys_all = jnp.dot(normed, key_weight, preferred_element_type=jnp.float32).astype(jnp.bfloat16)
    values = jnp.dot(normed, value_weight, preferred_element_type=jnp.float32).astype(jnp.bfloat16)
    positions = jnp.arange(length, dtype=jnp.float32)
    queries = rotate(queries.reshape(length, HEADS, 2, HEAD_DIM), positions)
    keys_all = rotate(keys_all.reshape(length, HEADS, 2, HEAD_DIM), positions)
    values = values.reshape(length, HEADS, 2 * HEAD_DIM)
    span = math.gcd(length, 512)

    def one_head(operands):
        query_head, key_head, value_head, lambda_head = operands
        key_float = key_head.astype(jnp.float32)
        value_float = value_head.astype(jnp.float32)

        def one_block(begin):
            query_block = lax.dynamic_slice_in_dim(query_head, begin, span, 0).astype(jnp.float32)
            scores = jnp.einsum('qcd,kcd->cqk', query_block, key_float) * HEAD_DIM ** (-0.5)
            query_pos = begin + jnp.arange(span, dtype=jnp.int32)
            key_pos = jnp.arange(length, dtype=jnp.int32)
            scores = jnp.where(query_pos[:, None] >= key_pos[None, :], scores, -jnp.inf)
            largest = lax.optimization_barrier(jnp.max(scores, -1, keepdims=True))
            expons = jnp.exp(scores - largest)
            totals = lax.optimization_barrier(jnp.sum(expons, -1))
            expons_low = expons.astype(jnp.bfloat16).astype(jnp.float32)
            map_values = jnp.einsum('cqk,ke->cqe', expons_low, value_float)
            return map_values[0] / totals[0][:, None] - lambda_head * map_values[1] / totals[1][:, None]
        begins = jnp.arange(length // span, dtype=jnp.int32) * span
        return lax.map(one_block, begins).reshape(length, 2 * HEAD_DIM)
    heads_raw = lax.map(one_head, (jnp.moveaxis(queries, 1, 0), jnp.moveaxis(keys_all, 1, 0), jnp.moveaxis(values, 1, 0), diff_lambda))
    heads_raw = jnp.moveaxis(heads_raw, 0, 1)
    attn = (heads_raw * lax.rsqrt(lax.optimization_barrier(jnp.mean(heads_raw * heads_raw, -1, keepdims=True)) + HEAD_EPS) * head_gain * HEAD_SCALE).astype(jnp.bfloat16).reshape(length, 2 * HEADS * HEAD_DIM)
    grouped = pool_in.reshape(length, POOL_GROUPS, GROUP_DIM).astype(jnp.float32)
    running = jnp.concatenate([jnp.zeros((1, POOL_GROUPS, GROUP_DIM), jnp.float32), jnp.cumsum(grouped, 0)], 0)
    windows = 2 ** (1 + jnp.arange(POOL_GROUPS, dtype=jnp.int32) % 4)
    places = jnp.arange(length, dtype=jnp.int32)[:, None]
    lowest = jnp.maximum(places + 1 - windows[None, :], 0)
    counts = jnp.minimum(places + 1, windows[None, :]).astype(jnp.float32)
    low_sums = running[lowest, jnp.arange(POOL_GROUPS, dtype=jnp.int32)[None, :]]
    window_mean = (running[1:] - low_sums) / counts[:, :, None]
    pool_mixed = (window_mean - grouped).astype(jnp.bfloat16)
    pooled = (jnp.einsum('sgc,gce->sge', pool_mixed.astype(jnp.float32), pool_map.astype(jnp.float32)) * pool_scale.reshape(POOL_GROUPS, GROUP_DIM)).astype(jnp.bfloat16).reshape(length, POOL_WIDTH)
    pool_cols = POOL_WIDTH // N_TP
    head_cols = 2 * HEADS * HEAD_DIM // N_TP
    summed = jnp.zeros((length, D), jnp.float32)
    for shard_index in range(N_TP):
        pool_part = pooled[:, shard_index * pool_cols:(shard_index + 1) * pool_cols]
        head_part = attn[:, shard_index * head_cols:(shard_index + 1) * head_cols]
        partial_value = jnp.dot(pool_part, out_pool[shard_index * pool_cols:(shard_index + 1) * pool_cols], preferred_element_type=jnp.float32) + jnp.dot(head_part, out_heads[shard_index * head_cols:(shard_index + 1) * head_cols], preferred_element_type=jnp.float32)
        rounded = lax.optimization_barrier(partial_value.astype(jnp.bfloat16))
        summed = summed + rounded.astype(jnp.float32)
    return summed.astype(jnp.bfloat16)

def reference(tokens, norm_gain, pool_input, query_weight, key_weight, value_weight, pool_map, pool_scale, head_gain, diff_lambda, out_pool, out_heads):

    def apply_one(seq_tokens):
        return one_sequence(seq_tokens, norm_gain, pool_input, query_weight, key_weight, value_weight, pool_map, pool_scale, head_gain, diff_lambda, out_pool, out_heads)
    return lax.map(apply_one, tokens)
```

```python
import math

import jax
import jax.numpy as jnp
from jax import lax
from jax.experimental import pallas as pl
from jax.experimental.pallas import tpu as pltpu
from jax.sharding import PartitionSpec as P

HEAD_DIM = 128
GROUP_DIM = 256


THETA = 500000.0
HEAD_SCALE = 0.8
NORM_EPS = 1e-06
HEAD_EPS = 1e-05


def from_behind(value, axis, steps):
    count = lax.axis_size(axis)
    first, last = (max(0, -steps), min(count, count - steps))
    return lax.ppermute(value, axis, [(source, source + steps) for source in range(first, last)])


def rotate(tensor, positions):
    half = HEAD_DIM // 2
    freqs = 1.0 / THETA ** (jnp.arange(half, dtype=jnp.float32) * 2.0 / HEAD_DIM)
    angles = positions[:, None] * freqs[None, :]
    cosine = jnp.cos(angles)[:, None, None, :]
    sine = jnp.sin(angles)[:, None, None, :]
    floated = tensor.astype(jnp.float32)
    first = floated[..., :half]
    second = floated[..., half:]
    turned = jnp.concatenate([first * cosine - second * sine, second * cosine + first * sine], -1)
    return turned.astype(jnp.bfloat16)


def local(
    tokens,
    norm_gain,
    pool_input,
    query_weight,
    key_weight,
    value_weight,
    pool_map,
    pool_scale,
    head_gain,
    diff_lambda,
    out_pool,
    out_heads,
):
    out_local = jnp.concatenate([out_pool, out_heads], 0)
    row_count = tokens.shape[1]
    floated = tokens[0].astype(jnp.float32)
    normed = (
        floated * lax.rsqrt(jnp.mean(floated * floated, -1, keepdims=True) + NORM_EPS) * norm_gain
    ).astype(jnp.bfloat16)
    fragments = (
        lax.all_gather(pool_input, ("sp", "fs"), axis=0, tiled=True),
        lax.all_gather(query_weight, ("sp", "fs"), axis=0, tiled=True),
        lax.all_gather(key_weight, ("sp", "fs"), axis=0, tiled=True),
        lax.all_gather(value_weight, ("sp", "fs"), axis=0, tiled=True),
    )
    projected = tuple(
        (jnp.dot(normed, fragment, preferred_element_type=jnp.float32) for fragment in fragments)
    )
    pool_in, queries, keys_flat, values_flat = [
        product.astype(jnp.bfloat16) for product in projected
    ]
    head_count = values_flat.shape[1] // (2 * HEAD_DIM)
    tp_index = lax.axis_index("tp")
    sp_index = lax.axis_index("sp")
    query_pos = sp_index * row_count + jnp.arange(row_count, dtype=jnp.int32)
    positions = query_pos.astype(jnp.float32)
    queries = rotate(queries.reshape(row_count, head_count, 2, HEAD_DIM), positions)
    keys_flat = rotate(keys_flat.reshape(row_count, head_count, 2, HEAD_DIM), positions).reshape(
        row_count, head_count * 2 * HEAD_DIM
    )
    lambdas = lax.dynamic_slice_in_dim(diff_lambda, tp_index * head_count, head_count, 0)

    def online_step(state, key_rows, value_rows, key_offset):
        largest, summed, accum = state
        width = key_rows.shape[0]
        shaped = key_rows.reshape(width, head_count, 2, HEAD_DIM)
        scores = jnp.einsum(
            "qhcd,khcd->chqk", queries, shaped, preferred_element_type=jnp.float32
        ) * HEAD_DIM ** (-0.5)
        key_pos = key_offset + jnp.arange(width, dtype=jnp.int32)
        scores = jnp.where(query_pos[:, None] >= key_pos[None, :], scores, -jnp.inf)
        newest = jnp.maximum(largest, jnp.max(scores, -1))
        anchor = jnp.where(jnp.isfinite(newest), newest, 0.0)
        rescale = jnp.exp(largest - anchor)
        expons = jnp.exp(scores - anchor[..., None])
        summed = summed * rescale + jnp.sum(expons, -1)
        value_shaped = value_rows.reshape(width, head_count, 2 * HEAD_DIM)
        added = jnp.einsum(
            "chqk,khe->chqe",
            expons.astype(jnp.bfloat16),
            value_shaped,
            preferred_element_type=jnp.float32,
        )
        accum = accum * rescale[..., None] + added
        return (newest, summed, accum)

    start_state = (
        jnp.full((2, head_count, row_count), -jnp.inf, jnp.float32),
        jnp.zeros((2, head_count, row_count), jnp.float32),
        jnp.zeros((2, head_count, row_count, 2 * HEAD_DIM), jnp.float32),
    )
    fragments = (
        lax.all_gather(keys_flat, "sp", axis=0, tiled=True),
        lax.all_gather(values_flat, "sp", axis=0, tiled=True),
    )
    span = math.gcd(fragments[0].shape[0], 1024)

    def inner_step(index, inner_state):
        key_rows = lax.dynamic_slice_in_dim(fragments[0], index * span, span, 0)
        value_rows = lax.dynamic_slice_in_dim(fragments[1], index * span, span, 0)
        return online_step(inner_state, key_rows, value_rows, index * span)

    final_state = lax.fori_loop(0, fragments[0].shape[0] // span, inner_step, start_state)
    summed_final = final_state[1]
    accum_final = final_state[2]
    heads_raw = (
        accum_final[0] / summed_final[0][..., None]
        - lambdas[:, None, None] * accum_final[1] / summed_final[1][..., None]
    )
    heads_raw = jnp.moveaxis(heads_raw, 0, 1)
    attn = (
        (
            heads_raw
            * lax.rsqrt(jnp.mean(heads_raw * heads_raw, -1, keepdims=True) + HEAD_EPS)
            * head_gain
            * HEAD_SCALE
        )
        .astype(jnp.bfloat16)
        .reshape(row_count, head_count * 2 * HEAD_DIM)
    )
    reach = 15
    rim_rows = from_behind(pool_in[row_count - reach :], "sp", 1)
    extended = jnp.concatenate([rim_rows, pool_in], 0).astype(jnp.float32)
    pair_sums = extended[1:] + extended[:-1]
    quad_sums = pair_sums[2:] + pair_sums[:-2]
    octet_sums = quad_sums[4:] + quad_sums[:-4]
    sixteen_sums = octet_sums[8:] + octet_sums[:-8]
    group_count = pool_in.shape[1] // GROUP_DIM
    stacked = jnp.stack(
        [
            pair_sums[14 : 14 + row_count],
            quad_sums[12 : 12 + row_count],
            octet_sums[8 : 8 + row_count],
            sixteen_sums,
        ],
        0,
    ).reshape(4, row_count, group_count, GROUP_DIM)
    levels = (tp_index * group_count + jnp.arange(group_count, dtype=jnp.int32)) % 4
    picked = jnp.sum(
        jnp.where(
            levels[None, None, :, None] == jnp.arange(4, dtype=jnp.int32)[:, None, None, None],
            stacked,
            0.0,
        ),
        0,
    )
    windows = 2 ** (1 + levels)
    counts = jnp.minimum(query_pos[:, None] + 1, windows[None, :]).astype(jnp.float32)
    window_mean = picked / counts[:, :, None]
    grouped = pool_in.reshape(row_count, group_count, GROUP_DIM).astype(jnp.float32)
    pool_mixed = (window_mean - grouped).astype(jnp.bfloat16)
    pooled = (
        (
            jnp.einsum("tgc,gce->tge", pool_mixed, pool_map, preferred_element_type=jnp.float32)
            * pool_scale.reshape(group_count, GROUP_DIM)
        )
        .astype(jnp.bfloat16)
        .reshape(row_count, group_count * GROUP_DIM)
    )
    branches = jnp.concatenate([pooled, attn], 1)
    partial_value = jnp.dot(
        branches,
        lax.all_gather(out_local, ("sp", "fs"), axis=1, tiled=True),
        preferred_element_type=jnp.float32,
    )
    layer_out = lax.psum_scatter(
        partial_value.astype(jnp.bfloat16), "tp", scatter_dimension=1, tiled=True
    )
    return layer_out[None]


MESH = pl.DeviceIdType.MESH

def fused_kernel(
    places,
    groups,
    normed_ref,
    pool_ref,
    query_ref,
    key_ref,
    value_ref,
    map_ref,
    scale_ref,
    gain_ref,
    lambda_ref,
    out_pool_ref,
    out_heads_ref,
    cos_ref,
    sin_ref,
    out_ref,
    rows_all,
    weights,
    outs,
    queries,
    keys,
    values,
    pools,
    to_mate,
    from_mate,
    to_peer,
    from_peer,
    *sems,
):
    (
        own_sem,
        in_local,
        in_z_send,
        in_z_recv,
        in_n_send,
        in_n_recv,
        in_f_send,
        in_f_recv,
        out_local,
        out_z_send,
        out_z_recv,
        out_n_send,
        out_n_recv,
        out_f_send,
        out_f_recv,
        right_send,
        right_recv,
        left_send,
        left_recv,
        mate_send,
        mate_recv,
        half_send,
        half_recv,
        peer_send,
        peer_recv,
    ) = sems
    z = lax.axis_index("sp")
    f = lax.axis_index("fs")
    c = lax.axis_index("tp")
    fx = f + 1 - 2 * lax.rem(f, 2)
    fy = lax.rem(f + 2, groups)
    mate = 1 - c
    half_rows = normed_ref.shape[0]
    row_count = 2 * half_rows
    depth = pool_ref.shape[0]
    width = GROUP_DIM
    out_width = out_pool_ref.shape[1]
    half_out = out_ref.shape[1]

    barrier = pltpu.get_barrier_semaphore()
    partners = [{"sp": lax.rem(z + d, places)} for d in range(1, places)]
    partners += [{"fs": fx}, {"fs": fy}, {"tp": mate}]
    for partner in partners:
        pl.semaphore_signal(barrier, inc=1, device_id=partner, device_id_type=MESH)
    pl.semaphore_wait(barrier, len(partners))

    def remote(source, target, send, recv, device):
        return pltpu.make_async_remote_copy(
            src_ref=source,
            dst_ref=target,
            send_sem=send,
            recv_sem=recv,
            device_id=device,
            device_id_type=MESH,
        )

    def block(index, size):
        return pl.ds(pl.multiple_of(index * size, size), size)

    class Gather:
        def __init__(self, sources, cut, view, group):
            self.sources, self.cut, self.view = sources, cut, view
            self.count = len(sources)
            (
                self.local,
                self.z_send,
                self.z_recv,
                self.n_send,
                self.n_recv,
                self.f_send,
                self.f_recv,
            ) = group
            self.low = (0, self.count // 2)
            self.high = (self.count // 2, self.count - self.count // 2)

        def own(self, m):
            return pltpu.make_async_copy(
                self.cut(self.sources[m], z), self.view(z, f, m, 1).at[0], self.local.at[m]
            )

        def across(self, d, m):
            to = lax.rem(z + d, places)
            return remote(
                self.cut(self.sources[m], to),
                self.view(z, f, m, 1).at[0],
                self.z_send.at[d, m],
                self.z_recv.at[d, m],
                {"sp": to},
            )

        def arrive(self, d, m):
            view = self.view(lax.rem(z + places - d, places), f, m, 1).at[0]
            return remote(
                view,
                view,
                self.z_send.at[d, m],
                self.z_recv.at[d, m],
                {"sp": lax.rem(z + places - d, places)},
            )

        def near(self, d, side, column):
            view = self.view(lax.rem(z + places - d, places), column, 0, self.count)
            return remote(
                view,
                view,
                self.n_send.at[side, d],
                self.n_recv.at[side, d],
                {"fs": (fx, fy)[side]},
            )

        def forward(self, d, side, column):
            start, size = (self.high, self.low)[side]
            view = self.view(lax.rem(z + places - d, places), column, start, size)
            return remote(
                view,
                view,
                self.f_send.at[side, d],
                self.f_recv.at[side, d],
                {"fs": (fx, fy)[side]},
            )

        def start(self):
            for m in range(self.count):
                self.own(m).start()
            for d in range(1, places):
                for m in range(self.count):
                    self.across(d, m).start()

        def first(self, d):
            for m in range(self.count):
                if d == 0:
                    self.own(m).wait()
                else:
                    self.arrive(d, m).wait_recv()
            for side in range(2):
                self.near(d, side, f).start()

        def second(self, d):
            self.near(d, 0, fx).wait_recv()
            self.forward(d, 1, fx).start()
            self.near(d, 1, fy).wait_recv()
            self.forward(d, 0, fy).start()

        def third(self, d):
            diagonal = lax.rem(fx + 2, groups)
            for side in range(2):
                self.forward(d, side, diagonal).wait_recv()

        def drain(self):
            for d in range(places):
                for m in range(self.count):
                    if d > 0:
                        self.across(d, m).wait_send()
                for side in range(2):
                    self.near(d, side, f).wait_send()
                self.forward(d, 1, fx).wait_send()
                self.forward(d, 0, fy).wait_send()

    inward = Gather(
        (pool_ref, query_ref, key_ref, value_ref),
        lambda ref, to: ref.at[:, block(to, width)],
        lambda zz, ff, m, n: weights.at[pl.ds(m, n), block(zz * groups + ff, depth), :],
        (in_local, in_z_send, in_z_recv, in_n_send, in_n_recv, in_f_send, in_f_recv),
    )
    outward = Gather(
        (out_pool_ref, out_heads_ref),
        lambda ref, to: ref.at[block(to, width), :],
        lambda zz, ff, m, n: outs.at[pl.ds(m, n), :, block(zz * groups + ff, out_width)],
        (out_local, out_z_send, out_z_recv, out_n_send, out_n_recv, out_f_send, out_f_recv),
    )

    def chunk(zz, side):
        return rows_all.at[block(2 * zz + side, half_rows), :]

    def right(k):
        view = chunk(z - k, c)
        return remote(view, view, right_send.at[k], right_recv.at[k + 1], {"sp": z + 1})

    def from_left(k):
        view = chunk(z - k, c)
        return remote(view, view, right_send.at[k], right_recv.at[k], {"sp": z - 1})

    def left(k):
        view = chunk(z + k, c)
        return remote(view, view, left_send.at[k], left_recv.at[k + 1], {"sp": z - 1})

    def from_right(k):
        view = chunk(z + k, c)
        return remote(view, view, left_send.at[k], left_recv.at[k], {"sp": z + 1})

    def share(slot, zz, side):
        view = chunk(zz, side)
        return remote(view, view, mate_send.at[slot], mate_recv.at[slot], {"tp": mate})

    own_rows = pltpu.make_async_copy(normed_ref, chunk(z, c), own_sem)
    own_rows.start()
    inward.start()
    own_rows.wait()

    @pl.when(z < places - 1)
    def _():
        right(0).start()

    @pl.when(z > 0)
    def _():
        left(0).start()

    share(0, z, c).start()

    def tokens_step(k):
        @pl.when(z >= k)
        def _():
            from_left(k).wait_recv()

            @pl.when(z < places - 1)
            def _():
                right(k).start()

            share(k, z - k, c).start()

        @pl.when(z + k < places)
        def _():
            from_right(k).wait_recv()

            @pl.when(z > 0)
            def _():
                left(k).start()

            share(places - 1 + k, z + k, c).start()

    for d in range(places):
        inward.first(d)
        if d > 0:
            inward.second(d - 1)
    pools[0:16, :] = jnp.zeros((16, width), jnp.bfloat16)
    tokens_step(1)
    inward.second(places - 1)
    for k in range(2, places):
        tokens_step(k)
    outward.start()
    for d in range(places):
        inward.third(d)

    share(0, z, mate).wait_recv()
    for k in range(1, places):

        @pl.when(z >= k)
        def _():
            share(k, z - k, mate).wait_recv()

        @pl.when(z + k < places)
        def _():
            share(places - 1 + k, z + k, mate).wait_recv()

    def turned(raw, cosine, sine):
        floated = raw.astype(jnp.float32)
        return (floated * cosine + pltpu.roll(floated, HEAD_DIM // 2, 1) * sine).astype(
            jnp.bfloat16
        )

    def project(index, carry):
        rows = block(index, row_count)
        normed = rows_all[rows, :]
        cosine = cos_ref[rows, :]
        sine = sin_ref[rows, :]

        def product(m):
            return jnp.dot(normed, weights[m], preferred_element_type=jnp.float32).astype(
                jnp.bfloat16
            )

        pools[pl.ds(pl.multiple_of(index * row_count + 16, 16), row_count), :] = product(0)
        raw = product(1)
        for m in range(2):
            part = slice(m * HEAD_DIM, (m + 1) * HEAD_DIM)
            queries[rows, part] = turned(raw[:, part], cosine, sine)
        raw = product(2)
        for m in range(2):
            part = slice(m * HEAD_DIM, (m + 1) * HEAD_DIM)
            keys[rows, part] = turned(raw[:, part], cosine, sine)
        values[rows, :] = product(3)
        return carry

    outward.first(0)
    lax.fori_loop(0, places, project, 0)
    for d in range(1, places):
        outward.first(d)
        outward.second(d - 1)
    outward.second(places - 1)
    for d in range(places):
        outward.third(d)

    level = lax.rem(c * map_ref.shape[0] + z, 4)
    window = jnp.where(
        level == 0, 2, jnp.where(level == 1, 4, jnp.where(level == 2, 8, 16))
    )
    head_lambda = lambda_ref[c * map_ref.shape[0] + z]
    length = places * row_count

    def to_sibling(d, to):
        return remote(
            to_mate.at[to], from_mate.at[to], half_send.at[d], half_recv.at[d], {"tp": mate}
        )

    def to_place(d, to):
        return remote(
            to_peer.at[to], from_peer.at[d], peer_send.at[d], peer_recv.at[d], {"sp": to}
        )

    def compute(step, carry):
        d = lax.rem(step + 1, places)
        to = lax.rem(z + d, places)
        rows = block(to, row_count)
        query_pos = to * row_count + lax.broadcasted_iota(jnp.int32, (row_count, length), 0)
        key_pos = lax.broadcasted_iota(jnp.int32, (row_count, length), 1)
        seen = query_pos >= key_pos
        mapped = []
        for m in range(2):
            part = slice(m * HEAD_DIM, (m + 1) * HEAD_DIM)
            scores = lax.dot_general(
                queries[rows, part],
                keys[:, part],
                (((1,), (1,)), ((), ())),
                preferred_element_type=jnp.float32,
            ) * HEAD_DIM ** (-0.5)
            scores = jnp.where(seen, scores, -jnp.inf)
            expons = jnp.exp(scores - jnp.max(scores, -1, keepdims=True))
            totals = jnp.sum(expons, -1, keepdims=True)
            mapped.append(
                jnp.dot(
                    expons.astype(jnp.bfloat16), values[...], preferred_element_type=jnp.float32
                )
                / totals
            )
        raw = mapped[0] - head_lambda * mapped[1]
        attn = (
            raw
            * lax.rsqrt(jnp.mean(raw * raw, -1, keepdims=True) + HEAD_EPS)
            * gain_ref[...]
            * HEAD_SCALE
        ).astype(jnp.bfloat16)
        extended = pools[
            pl.ds(pl.multiple_of(to * row_count, 16), row_count + 16), :
        ].astype(jnp.float32)
        picked = extended + pltpu.roll(extended, 1, 0)
        sums = picked
        for shift in (2, 4, 8):
            sums = sums + pltpu.roll(sums, shift, 0)
            picked = lax.select_n(window >= 2 * shift, picked, sums)
        places_of = to * row_count + lax.broadcasted_iota(jnp.int32, (row_count, 1), 0)
        counts = jnp.minimum(places_of + 1, window).astype(jnp.float32)
        mixed = (picked[16:] / counts - extended[16:]).astype(jnp.bfloat16)
        pooled = (
            jnp.dot(mixed, map_ref[z], preferred_element_type=jnp.float32) * scale_ref[z]
        ).astype(jnp.bfloat16)

        def partial_of(side):
            columns = block(side, half_out)
            return jnp.dot(
                pooled, outs[0, :, columns], preferred_element_type=jnp.float32
            ) + jnp.dot(attn, outs[1, :, columns], preferred_element_type=jnp.float32)

        to_mate[to] = partial_of(mate).astype(jnp.bfloat16)
        to_sibling(d, to).start()
        mine = partial_of(c)
        to_sibling(d, to).wait_recv()
        summed = mine + from_mate[to].astype(jnp.float32)

        to_peer[to] = summed.astype(jnp.bfloat16)

        @pl.when(d > 0)
        def _():
            to_place(d, to).start()

        return carry

    lax.fori_loop(0, places, compute, 0)

    total = to_peer[z].astype(jnp.float32)
    for d in range(1, places):
        to_place(d, lax.rem(z + d, places)).wait_recv()
        total = total + from_peer[d].astype(jnp.float32)
    out_ref[...] = total.astype(out_ref.dtype)

    inward.drain()
    outward.drain()

    @pl.when(z < places - 1)
    def _():
        right(0).wait_send()

    @pl.when(z > 0)
    def _():
        left(0).wait_send()

    share(0, z, c).wait_send()
    for k in range(1, places):

        @pl.when(z >= k)
        def _():
            @pl.when(z < places - 1)
            def _():
                right(k).wait_send()

            share(k, z - k, c).wait_send()

        @pl.when(z + k < places)
        def _():
            @pl.when(z > 0)
            def _():
                left(k).wait_send()

            share(places - 1 + k, z + k, c).wait_send()

    for d in range(places):
        to = lax.rem(z + d, places)
        to_sibling(d, to).wait_send()
        if d > 0:
            to_place(d, to).wait_send()


def fused(
    tokens,
    norm_gain,
    pool_input,
    query_weight,
    key_weight,
    value_weight,
    pool_map,
    pool_scale,
    head_gain,
    diff_lambda,
    out_pool,
    out_heads,
):
    places = lax.axis_size("sp")
    groups = lax.axis_size("fs")
    row_count, model = tokens.shape[1], tokens.shape[2]
    half_rows = row_count // 2
    floated = lax.dynamic_slice_in_dim(
        tokens[0], lax.axis_index("tp") * half_rows, half_rows, 0
    ).astype(jnp.float32)
    normed = (
        floated * lax.rsqrt(jnp.mean(floated * floated, -1, keepdims=True) + NORM_EPS) * norm_gain
    ).astype(jnp.bfloat16)
    length = places * row_count
    half = HEAD_DIM // 2
    freqs = 1.0 / THETA ** (jnp.arange(half, dtype=jnp.float32) * 2.0 / HEAD_DIM)
    angles = jnp.arange(length, dtype=jnp.float32)[:, None] * freqs[None, :]
    cosine, sine = jnp.cos(angles), jnp.sin(angles)
    cosine = jnp.concatenate([cosine, cosine], 1)
    sine = jnp.concatenate([-sine, sine], 1)
    group_count = pool_map.shape[0]
    half_out = model // 2
    vmem = pl.BlockSpec(memory_space=pltpu.VMEM)
    smem = pl.BlockSpec(memory_space=pltpu.SMEM)
    dma = pltpu.SemaphoreType.DMA
    low = jnp.bfloat16

    def gather_sems(count):
        return [
            dma((count,)),
            dma((places, count)),
            dma((places, count)),
            dma((2, places)),
            dma((2, places)),
            dma((2, places)),
            dma((2, places)),
        ]

    out = pl.pallas_call(
        lambda *refs: fused_kernel(places, groups, *refs),
        out_shape=jax.ShapeDtypeStruct((row_count, half_out), low),
        in_specs=[vmem] * 8 + [smem] + [vmem] * 4,
        out_specs=vmem,
        scratch_shapes=[
            pltpu.VMEM((length, model), low),
            pltpu.VMEM((4, model, GROUP_DIM), low),
            pltpu.VMEM((2, GROUP_DIM, model), low),
            pltpu.VMEM((length, GROUP_DIM), low),
            pltpu.VMEM((length, GROUP_DIM), low),
            pltpu.VMEM((length, GROUP_DIM), low),
            pltpu.VMEM((length + 16, GROUP_DIM), low),
            pltpu.VMEM((places, row_count, half_out), low),
            pltpu.VMEM((places, row_count, half_out), low),
            pltpu.VMEM((places, row_count, half_out), low),
            pltpu.VMEM((places, row_count, half_out), low),
            dma,
            *gather_sems(4),
            *gather_sems(2),
            dma((places,)),
            dma((places + 1,)),
            dma((places,)),
            dma((places + 1,)),
            dma((2 * places,)),
            dma((2 * places,)),
            dma((places,)),
            dma((places,)),
            dma((places,)),
            dma((places,)),
        ],
        compiler_params=pltpu.CompilerParams(
            collective_id=0, has_side_effects=True, vmem_limit_bytes=56 * 1024 * 1024
        ),
    )(
        normed,
        pool_input,
        query_weight,
        key_weight,
        value_weight,
        pool_map,
        pool_scale.reshape(group_count, 1, GROUP_DIM),
        head_gain.reshape(1, 2 * HEAD_DIM),
        diff_lambda,
        out_pool,
        out_heads,
        cosine,
        sine,
    )
    return out[None]


def solution(mesh):
    placed = (
        P("fs", "sp", None),
        P(),
        P(("sp", "fs"), "tp"),
        P(("sp", "fs"), "tp"),
        P(("sp", "fs"), "tp"),
        P(("sp", "fs"), "tp"),
        P("tp", None, None),
        P("tp"),
        P(),
        P(),
        P("tp", ("sp", "fs")),
        P("tp", ("sp", "fs")),
    )
    shape = dict(mesh.shape)

    def body(tokens, *rest):
        head_count = rest[3].shape[1] // (2 * HEAD_DIM)
        group_count = rest[5].shape[0]
        fits = (
            shape["fs"] == 4
            and shape["tp"] == 2
            and shape["sp"] == head_count == group_count
            and tokens.shape[0] == 1
        )
        return (fused if fits else local)(tokens, *rest)

    return jax.shard_map(
        body, mesh=mesh, in_specs=placed, out_specs=P("fs", "sp", "tp"), check_vma=False
    )
```

```python
import math

import jax
import jax.numpy as jnp
from jax import lax
from jax.experimental import pallas as pl
from jax.experimental.pallas import tpu as pltpu
from jax.sharding import PartitionSpec as P

HEAD_DIM = 128
GROUP_DIM = 256


THETA = 500000.0
HEAD_SCALE = 0.8
NORM_EPS = 1e-06
HEAD_EPS = 1e-05


def from_behind(value, axis, steps):
    count = lax.axis_size(axis)
    first, last = (max(0, -steps), min(count, count - steps))
    return lax.ppermute(value, axis, [(source, source + steps) for source in range(first, last)])


def rotate(tensor, positions):
    half = HEAD_DIM // 2
    freqs = 1.0 / THETA ** (jnp.arange(half, dtype=jnp.float32) * 2.0 / HEAD_DIM)
    angles = positions[:, None] * freqs[None, :]
    cosine = jnp.cos(angles)[:, None, None, :]
    sine = jnp.sin(angles)[:, None, None, :]
    floated = tensor.astype(jnp.float32)
    first = floated[..., :half]
    second = floated[..., half:]
    turned = jnp.concatenate([first * cosine - second * sine, second * cosine + first * sine], -1)
    return turned.astype(jnp.bfloat16)


def local(
    tokens,
    norm_gain,
    pool_input,
    query_weight,
    key_weight,
    value_weight,
    pool_map,
    pool_scale,
    head_gain,
    diff_lambda,
    out_pool,
    out_heads,
):
    out_local = jnp.concatenate([out_pool, out_heads], 0)
    row_count = tokens.shape[1]
    floated = tokens[0].astype(jnp.float32)
    normed = (
        floated * lax.rsqrt(jnp.mean(floated * floated, -1, keepdims=True) + NORM_EPS) * norm_gain
    ).astype(jnp.bfloat16)
    fragments = (
        lax.all_gather(pool_input, ("sp", "fs"), axis=0, tiled=True),
        lax.all_gather(query_weight, ("sp", "fs"), axis=0, tiled=True),
        lax.all_gather(key_weight, ("sp", "fs"), axis=0, tiled=True),
        lax.all_gather(value_weight, ("sp", "fs"), axis=0, tiled=True),
    )
    projected = tuple(
        (jnp.dot(normed, fragment, preferred_element_type=jnp.float32) for fragment in fragments)
    )
    pool_in, queries, keys_flat, values_flat = [
        product.astype(jnp.bfloat16) for product in projected
    ]
    head_count = values_flat.shape[1] // (2 * HEAD_DIM)
    tp_index = lax.axis_index("tp")
    sp_index = lax.axis_index("sp")
    query_pos = sp_index * row_count + jnp.arange(row_count, dtype=jnp.int32)
    positions = query_pos.astype(jnp.float32)
    queries = rotate(queries.reshape(row_count, head_count, 2, HEAD_DIM), positions)
    keys_flat = rotate(keys_flat.reshape(row_count, head_count, 2, HEAD_DIM), positions).reshape(
        row_count, head_count * 2 * HEAD_DIM
    )
    lambdas = lax.dynamic_slice_in_dim(diff_lambda, tp_index * head_count, head_count, 0)

    def online_step(state, key_rows, value_rows, key_offset):
        largest, summed, accum = state
        width = key_rows.shape[0]
        shaped = key_rows.reshape(width, head_count, 2, HEAD_DIM)
        scores = jnp.einsum(
            "qhcd,khcd->chqk", queries, shaped, preferred_element_type=jnp.float32
        ) * HEAD_DIM ** (-0.5)
        key_pos = key_offset + jnp.arange(width, dtype=jnp.int32)
        scores = jnp.where(query_pos[:, None] >= key_pos[None, :], scores, -jnp.inf)
        newest = jnp.maximum(largest, jnp.max(scores, -1))
        anchor = jnp.where(jnp.isfinite(newest), newest, 0.0)
        rescale = jnp.exp(largest - anchor)
        expons = jnp.exp(scores - anchor[..., None])
        summed = summed * rescale + jnp.sum(expons, -1)
        value_shaped = value_rows.reshape(width, head_count, 2 * HEAD_DIM)
        added = jnp.einsum(
            "chqk,khe->chqe",
            expons.astype(jnp.bfloat16),
            value_shaped,
            preferred_element_type=jnp.float32,
        )
        accum = accum * rescale[..., None] + added
        return (newest, summed, accum)

    start_state = (
        jnp.full((2, head_count, row_count), -jnp.inf, jnp.float32),
        jnp.zeros((2, head_count, row_count), jnp.float32),
        jnp.zeros((2, head_count, row_count, 2 * HEAD_DIM), jnp.float32),
    )
    fragments = (
        lax.all_gather(keys_flat, "sp", axis=0, tiled=True),
        lax.all_gather(values_flat, "sp", axis=0, tiled=True),
    )
    span = math.gcd(fragments[0].shape[0], 1024)

    def inner_step(index, inner_state):
        key_rows = lax.dynamic_slice_in_dim(fragments[0], index * span, span, 0)
        value_rows = lax.dynamic_slice_in_dim(fragments[1], index * span, span, 0)
        return online_step(inner_state, key_rows, value_rows, index * span)

    final_state = lax.fori_loop(0, fragments[0].shape[0] // span, inner_step, start_state)
    summed_final = final_state[1]
    accum_final = final_state[2]
    heads_raw = (
        accum_final[0] / summed_final[0][..., None]
        - lambdas[:, None, None] * accum_final[1] / summed_final[1][..., None]
    )
    heads_raw = jnp.moveaxis(heads_raw, 0, 1)
    attn = (
        (
            heads_raw
            * lax.rsqrt(jnp.mean(heads_raw * heads_raw, -1, keepdims=True) + HEAD_EPS)
            * head_gain
            * HEAD_SCALE
        )
        .astype(jnp.bfloat16)
        .reshape(row_count, head_count * 2 * HEAD_DIM)
    )
    reach = 15
    rim_rows = from_behind(pool_in[row_count - reach :], "sp", 1)
    extended = jnp.concatenate([rim_rows, pool_in], 0).astype(jnp.float32)
    pair_sums = extended[1:] + extended[:-1]
    quad_sums = pair_sums[2:] + pair_sums[:-2]
    octet_sums = quad_sums[4:] + quad_sums[:-4]
    sixteen_sums = octet_sums[8:] + octet_sums[:-8]
    group_count = pool_in.shape[1] // GROUP_DIM
    stacked = jnp.stack(
        [
            pair_sums[14 : 14 + row_count],
            quad_sums[12 : 12 + row_count],
            octet_sums[8 : 8 + row_count],
            sixteen_sums,
        ],
        0,
    ).reshape(4, row_count, group_count, GROUP_DIM)
    levels = (tp_index * group_count + jnp.arange(group_count, dtype=jnp.int32)) % 4
    picked = jnp.sum(
        jnp.where(
            levels[None, None, :, None] == jnp.arange(4, dtype=jnp.int32)[:, None, None, None],
            stacked,
            0.0,
        ),
        0,
    )
    windows = 2 ** (1 + levels)
    counts = jnp.minimum(query_pos[:, None] + 1, windows[None, :]).astype(jnp.float32)
    window_mean = picked / counts[:, :, None]
    grouped = pool_in.reshape(row_count, group_count, GROUP_DIM).astype(jnp.float32)
    pool_mixed = (window_mean - grouped).astype(jnp.bfloat16)
    pooled = (
        (
            jnp.einsum("tgc,gce->tge", pool_mixed, pool_map, preferred_element_type=jnp.float32)
            * pool_scale.reshape(group_count, GROUP_DIM)
        )
        .astype(jnp.bfloat16)
        .reshape(row_count, group_count * GROUP_DIM)
    )
    branches = jnp.concatenate([pooled, attn], 1)
    partial_value = jnp.dot(
        branches,
        lax.all_gather(out_local, ("sp", "fs"), axis=1, tiled=True),
        preferred_element_type=jnp.float32,
    )
    layer_out = lax.psum_scatter(
        partial_value.astype(jnp.bfloat16), "tp", scatter_dimension=1, tiled=True
    )
    return layer_out[None]


MESH = pl.DeviceIdType.MESH
PIECES = 2

def fused_kernel(
    places,
    groups,
    normed_ref,
    pool_ref,
    query_ref,
    key_ref,
    value_ref,
    map_ref,
    scale_ref,
    gain_ref,
    lambda_ref,
    out_pool_ref,
    out_heads_ref,
    cos_ref,
    sin_ref,
    out_ref,
    rows_all,
    weights,
    outs,
    queries,
    keys,
    values,
    pools,
    to_mate,
    from_mate,
    to_peer,
    from_peer,
    merging,
    final,
    *sems,
):
    (
        own_sem,
        in_local,
        in_z_send,
        in_z_recv,
        in_n_send,
        in_n_recv,
        in_f_send,
        in_f_recv,
        out_local,
        out_z_send,
        out_z_recv,
        out_n_send,
        out_n_recv,
        out_f_send,
        out_f_recv,
        right_send,
        right_recv,
        left_send,
        left_recv,
        mate_send,
        mate_recv,
        half_send,
        half_recv,
        peer_send,
        peer_recv,
        merge_send,
        merge_recv,
    ) = sems
    z = lax.axis_index("sp")
    f = lax.axis_index("fs")
    c = lax.axis_index("tp")
    fx = f + 1 - 2 * lax.rem(f, 2)
    fy = lax.rem(f + 2, groups)
    mate = 1 - c
    half_rows = normed_ref.shape[0]
    row_count = 2 * half_rows
    depth = pool_ref.shape[0]
    width = GROUP_DIM
    out_width = out_pool_ref.shape[1]
    half_out = out_ref.shape[1]

    barrier = pltpu.get_barrier_semaphore()
    partners = [{"sp": lax.rem(z + d, places)} for d in range(1, places)]
    partners += [{"fs": fx}, {"fs": fy}, {"tp": mate}]
    for partner in partners:
        pl.semaphore_signal(barrier, inc=1, device_id=partner, device_id_type=MESH)
    pl.semaphore_wait(barrier, len(partners))

    def remote(source, target, send, recv, device):
        return pltpu.make_async_remote_copy(
            src_ref=source,
            dst_ref=target,
            send_sem=send,
            recv_sem=recv,
            device_id=device,
            device_id_type=MESH,
        )

    def block(index, size):
        return pl.ds(pl.multiple_of(index * size, size), size)

    class Gather:
        def __init__(self, sources, cut, view, group):
            self.sources, self.cut, self.view = sources, cut, view
            self.count = len(sources)
            (
                self.local,
                self.z_send,
                self.z_recv,
                self.n_send,
                self.n_recv,
                self.f_send,
                self.f_recv,
            ) = group
            self.low = (0, self.count // 2)
            self.high = (self.count // 2, self.count - self.count // 2)

        def own(self, m):
            return pltpu.make_async_copy(
                self.cut(self.sources[m], z), self.view(z, f, m, 1).at[0], self.local.at[m]
            )

        def across(self, d, m):
            to = lax.rem(z + d, places)
            return remote(
                self.cut(self.sources[m], to),
                self.view(z, f, m, 1).at[0],
                self.z_send.at[d, m],
                self.z_recv.at[d, m],
                {"sp": to},
            )

        def arrive(self, d, m):
            view = self.view(lax.rem(z + places - d, places), f, m, 1).at[0]
            return remote(
                view,
                view,
                self.z_send.at[d, m],
                self.z_recv.at[d, m],
                {"sp": lax.rem(z + places - d, places)},
            )

        def near(self, d, side, column):
            view = self.view(lax.rem(z + places - d, places), column, 0, self.count)
            return remote(
                view,
                view,
                self.n_send.at[side, d],
                self.n_recv.at[side, d],
                {"fs": (fx, fy)[side]},
            )

        def forward(self, d, side, column):
            start, size = (self.high, self.low)[side]
            view = self.view(lax.rem(z + places - d, places), column, start, size)
            return remote(
                view,
                view,
                self.f_send.at[side, d],
                self.f_recv.at[side, d],
                {"fs": (fx, fy)[side]},
            )

        def start(self):
            for m in range(self.count):
                self.own(m).start()
            for d in range(1, places):
                for m in range(self.count):
                    self.across(d, m).start()

        def first(self, d):
            for m in range(self.count):
                if d == 0:
                    self.own(m).wait()
                else:
                    self.arrive(d, m).wait_recv()
            for side in range(2):
                self.near(d, side, f).start()

        def second(self, d):
            self.near(d, 0, fx).wait_recv()
            self.forward(d, 1, fx).start()
            self.near(d, 1, fy).wait_recv()
            self.forward(d, 0, fy).start()

        def third(self, d):
            diagonal = lax.rem(fx + 2, groups)
            for side in range(2):
                self.forward(d, side, diagonal).wait_recv()

        def drain(self):
            for d in range(places):
                for m in range(self.count):
                    if d > 0:
                        self.across(d, m).wait_send()
                for side in range(2):
                    self.near(d, side, f).wait_send()
                self.forward(d, 1, fx).wait_send()
                self.forward(d, 0, fy).wait_send()

    inward = Gather(
        (pool_ref, query_ref, key_ref, value_ref),
        lambda ref, to: ref.at[:, block(to, width)],
        lambda zz, ff, m, n: weights.at[pl.ds(m, n), block(zz * groups + ff, depth), :],
        (in_local, in_z_send, in_z_recv, in_n_send, in_n_recv, in_f_send, in_f_recv),
    )
    outward = Gather(
        (out_pool_ref, out_heads_ref),
        lambda ref, to: ref.at[block(to, width), :],
        lambda zz, ff, m, n: outs.at[pl.ds(m, n), :, block(zz * groups + ff, out_width)],
        (out_local, out_z_send, out_z_recv, out_n_send, out_n_recv, out_f_send, out_f_recv),
    )

    piece_rows = half_rows // PIECES

    def chunk(zz, side, p):
        return rows_all.at[block((2 * zz + side) * PIECES + p, piece_rows), :]

    def right(k, p):
        view = chunk(z - k, c, p)
        return remote(view, view, right_send.at[k, p], right_recv.at[k + 1, p], {"sp": z + 1})

    def from_left(k, p):
        view = chunk(z - k, c, p)
        return remote(view, view, right_send.at[k, p], right_recv.at[k, p], {"sp": z - 1})

    def left(k, p):
        view = chunk(z + k, c, p)
        return remote(view, view, left_send.at[k, p], left_recv.at[k + 1, p], {"sp": z - 1})

    def from_right(k, p):
        view = chunk(z + k, c, p)
        return remote(view, view, left_send.at[k, p], left_recv.at[k, p], {"sp": z + 1})

    def share(slot, zz, side, p):
        view = chunk(zz, side, p)
        return remote(view, view, mate_send.at[slot, p], mate_recv.at[slot, p], {"tp": mate})

    own_rows = pltpu.make_async_copy(
        normed_ref, rows_all.at[block(2 * z + c, half_rows), :], own_sem
    )
    own_rows.start()
    inward.start()
    outward.start()
    own_rows.wait()

    @pl.when(z < places - 1)
    def _():
        for p in range(PIECES):
            right(0, p).start()

    @pl.when(z > 0)
    def _():
        for p in range(PIECES):
            left(0, p).start()

    for p in range(PIECES):
        share(0, z, c, p).start()

    def tokens_step(k):
        for p in range(PIECES):

            @pl.when(z >= k)
            def _():
                from_left(k, p).wait_recv()

                @pl.when(z < places - 1)
                def _():
                    right(k, p).start()

                share(k, z - k, c, p).start()

            @pl.when(z + k < places)
            def _():
                from_right(k, p).wait_recv()

                @pl.when(z > 0)
                def _():
                    left(k, p).start()

                share(places - 1 + k, z + k, c, p).start()

    pools[0:16, :] = jnp.zeros((16, width), jnp.bfloat16)
    for d in range(places):
        inward.first(d)
        if d > 0:
            inward.second(d - 1)
    outward.first(0)
    inward.second(places - 1)
    for d in range(1, places):
        outward.first(d)
        if d > 1:
            outward.second(d - 2)
    tokens_step(1)
    for d in (places - 2, places - 1):
        outward.second(d)
    for k in range(2, places):
        tokens_step(k)
    for d in range(places):
        inward.third(d)

    for p in range(PIECES):
        share(0, z, mate, p).wait_recv()
        for k in range(1, places):

            @pl.when(z >= k)
            def _():
                share(k, z - k, mate, p).wait_recv()

            @pl.when(z + k < places)
            def _():
                share(places - 1 + k, z + k, mate, p).wait_recv()

    def turned(raw, cosine, sine):
        floated = raw.astype(jnp.float32)
        return (floated * cosine + pltpu.roll(floated, HEAD_DIM // 2, 1) * sine).astype(
            jnp.bfloat16
        )

    def project(index, carry):
        rows = block(index, row_count)
        normed = rows_all[rows, :]
        cosine = cos_ref[rows, :]
        sine = sin_ref[rows, :]

        def product(m):
            return jnp.dot(normed, weights[m], preferred_element_type=jnp.float32).astype(
                jnp.bfloat16
            )

        pools[pl.ds(pl.multiple_of(index * row_count + 16, 16), row_count), :] = product(0)
        raw = product(1)
        for m in range(2):
            part = slice(m * HEAD_DIM, (m + 1) * HEAD_DIM)
            queries[rows, part] = turned(raw[:, part], cosine, sine)
        raw = product(2)
        for m in range(2):
            part = slice(m * HEAD_DIM, (m + 1) * HEAD_DIM)
            keys[rows, part] = turned(raw[:, part], cosine, sine)
        values[rows, :] = product(3)
        return carry

    lax.fori_loop(0, places, project, 0)
    for d in range(places):
        outward.third(d)

    level = lax.rem(c * map_ref.shape[0] + z, 4)
    window = jnp.where(
        level == 0, 2, jnp.where(level == 1, 4, jnp.where(level == 2, 8, 16))
    )
    head_lambda = lambda_ref[c * map_ref.shape[0] + z]
    length = places * row_count

    def to_sibling(d, to):
        return remote(
            to_mate.at[to], from_mate.at[to], half_send.at[d], half_recv.at[d], {"tp": mate}
        )

    outer = (z == 0) | (z == places - 1)
    pair = z + 1 - 2 * lax.rem(z, 2)
    far = jnp.where(z < 2, places - 1, 0)
    near = jnp.where(z < 2, 2, 1)

    def to_inner(role, to):
        return remote(
            to_peer.at[to], merging.at[role], merge_send.at[role], merge_recv.at[role], {"sp": pair}
        )

    def to_place(role, to):
        return remote(
            to_peer.at[to], from_peer.at[0], peer_send.at[role], peer_recv.at[0], {"sp": to}
        )

    def to_pair():
        return remote(
            to_peer.at[pair], from_peer.at[1], peer_send.at[2], peer_recv.at[1], {"sp": pair}
        )

    def compute(step, carry):
        role = jnp.where((step == 3) | outer, step, lax.rem(step + 2, 3))
        to = jnp.where(role == 0, far, jnp.where(role == 1, near, jnp.where(role == 2, pair, z)))
        d = step
        rows = block(to, row_count)
        query_pos = to * row_count + lax.broadcasted_iota(jnp.int32, (row_count, length), 0)
        key_pos = lax.broadcasted_iota(jnp.int32, (row_count, length), 1)
        seen = query_pos >= key_pos
        mapped = []
        for m in range(2):
            part = slice(m * HEAD_DIM, (m + 1) * HEAD_DIM)
            scores = lax.dot_general(
                queries[rows, part],
                keys[:, part],
                (((1,), (1,)), ((), ())),
                preferred_element_type=jnp.float32,
            ) * HEAD_DIM ** (-0.5)
            scores = jnp.where(seen, scores, -jnp.inf)
            expons = jnp.exp(scores - jnp.max(scores, -1, keepdims=True))
            totals = jnp.sum(expons, -1, keepdims=True)
            mapped.append(
                jnp.dot(
                    expons.astype(jnp.bfloat16), values[...], preferred_element_type=jnp.float32
                )
                / totals
            )
        raw = mapped[0] - head_lambda * mapped[1]
        attn = (
            raw
            * lax.rsqrt(jnp.mean(raw * raw, -1, keepdims=True) + HEAD_EPS)
            * gain_ref[...]
            * HEAD_SCALE
        ).astype(jnp.bfloat16)
        extended = pools[
            pl.ds(pl.multiple_of(to * row_count, 16), row_count + 16), :
        ].astype(jnp.float32)
        picked = extended + pltpu.roll(extended, 1, 0)
        sums = picked
        for shift in (2, 4, 8):
            sums = sums + pltpu.roll(sums, shift, 0)
            picked = lax.select_n(window >= 2 * shift, picked, sums)
        places_of = to * row_count + lax.broadcasted_iota(jnp.int32, (row_count, 1), 0)
        counts = jnp.minimum(places_of + 1, window).astype(jnp.float32)
        mixed = (picked[16:] / counts - extended[16:]).astype(jnp.bfloat16)
        pooled = (
            jnp.dot(mixed, map_ref[z], preferred_element_type=jnp.float32) * scale_ref[z]
        ).astype(jnp.bfloat16)

        def partial_of(side):
            columns = block(side, half_out)
            return jnp.dot(
                pooled, outs[0, :, columns], preferred_element_type=jnp.float32
            ) + jnp.dot(attn, outs[1, :, columns], preferred_element_type=jnp.float32)

        to_mate[to] = partial_of(mate).astype(jnp.bfloat16)
        to_sibling(d, to).start()
        mine = partial_of(c)
        to_sibling(d, to).wait_recv()
        summed = mine + from_mate[to].astype(jnp.float32)

        @pl.when((role < 2) & outer)
        def _():
            to_peer[to] = summed.astype(jnp.bfloat16)
            to_inner(role, to).start()

        @pl.when((role < 2) & jnp.logical_not(outer))
        def _():
            to_inner(role, to).wait_recv()
            to_peer[to] = (summed + merging[role].astype(jnp.float32)).astype(jnp.bfloat16)
            to_place(role, to).start()

        @pl.when(role == 2)
        def _():
            to_peer[to] = summed.astype(jnp.bfloat16)
            to_pair().start()

        @pl.when(role == 3)
        def _():
            final[...] = summed

        return carry

    lax.fori_loop(0, places, compute, 0)

    to_pair().wait_recv()
    total = final[...] + from_peer[1].astype(jnp.float32)
    to_place(0, z).wait_recv()
    out_ref[...] = (total + from_peer[0].astype(jnp.float32)).astype(out_ref.dtype)

    inward.drain()
    outward.drain()

    for p in range(PIECES):

        @pl.when(z < places - 1)
        def _():
            right(0, p).wait_send()

        @pl.when(z > 0)
        def _():
            left(0, p).wait_send()

        share(0, z, c, p).wait_send()
        for k in range(1, places):

            @pl.when(z >= k)
            def _():
                @pl.when(z < places - 1)
                def _():
                    right(k, p).wait_send()

                share(k, z - k, c, p).wait_send()

            @pl.when(z + k < places)
            def _():
                @pl.when(z > 0)
                def _():
                    left(k, p).wait_send()

                share(places - 1 + k, z + k, c, p).wait_send()

    for d in range(places):
        to_sibling(d, d).wait_send()
    for role, to in ((0, far), (1, near)):

        @pl.when(outer)
        def _():
            to_inner(role, to).wait_send()

        @pl.when(jnp.logical_not(outer))
        def _():
            to_place(role, to).wait_send()

    to_pair().wait_send()


def fused(
    tokens,
    norm_gain,
    pool_input,
    query_weight,
    key_weight,
    value_weight,
    pool_map,
    pool_scale,
    head_gain,
    diff_lambda,
    out_pool,
    out_heads,
):
    places = lax.axis_size("sp")
    groups = lax.axis_size("fs")
    row_count, model = tokens.shape[1], tokens.shape[2]
    half_rows = row_count // 2
    floated = lax.dynamic_slice_in_dim(
        tokens[0], lax.axis_index("tp") * half_rows, half_rows, 0
    ).astype(jnp.float32)
    normed = (
        floated * lax.rsqrt(jnp.mean(floated * floated, -1, keepdims=True) + NORM_EPS) * norm_gain
    ).astype(jnp.bfloat16)
    length = places * row_count
    half = HEAD_DIM // 2
    freqs = 1.0 / THETA ** (jnp.arange(half, dtype=jnp.float32) * 2.0 / HEAD_DIM)
    angles = jnp.arange(length, dtype=jnp.float32)[:, None] * freqs[None, :]
    cosine, sine = jnp.cos(angles), jnp.sin(angles)
    cosine = jnp.concatenate([cosine, cosine], 1)
    sine = jnp.concatenate([-sine, sine], 1)
    group_count = pool_map.shape[0]
    half_out = model // 2
    vmem = pl.BlockSpec(memory_space=pltpu.VMEM)
    smem = pl.BlockSpec(memory_space=pltpu.SMEM)
    dma = pltpu.SemaphoreType.DMA
    low = jnp.bfloat16

    def gather_sems(count):
        return [
            dma((count,)),
            dma((places, count)),
            dma((places, count)),
            dma((2, places)),
            dma((2, places)),
            dma((2, places)),
            dma((2, places)),
        ]

    out = pl.pallas_call(
        lambda *refs: fused_kernel(places, groups, *refs),
        out_shape=jax.ShapeDtypeStruct((row_count, half_out), low),
        in_specs=[vmem] * 8 + [smem] + [vmem] * 4,
        out_specs=vmem,
        scratch_shapes=[
            pltpu.VMEM((length, model), low),
            pltpu.VMEM((4, model, GROUP_DIM), low),
            pltpu.VMEM((2, GROUP_DIM, model), low),
            pltpu.VMEM((length, GROUP_DIM), low),
            pltpu.VMEM((length, GROUP_DIM), low),
            pltpu.VMEM((length, GROUP_DIM), low),
            pltpu.VMEM((length + 16, GROUP_DIM), low),
            pltpu.VMEM((places, row_count, half_out), low),
            pltpu.VMEM((places, row_count, half_out), low),
            pltpu.VMEM((places, row_count, half_out), low),
            pltpu.VMEM((2, row_count, half_out), low),
            pltpu.VMEM((2, row_count, half_out), low),
            pltpu.VMEM((row_count, half_out), jnp.float32),
            dma,
            *gather_sems(4),
            *gather_sems(2),
            dma((places, PIECES)),
            dma((places + 1, PIECES)),
            dma((places, PIECES)),
            dma((places + 1, PIECES)),
            dma((2 * places, PIECES)),
            dma((2 * places, PIECES)),
            dma((places,)),
            dma((places,)),
            dma((3,)),
            dma((2,)),
            dma((2,)),
            dma((2,)),
        ],
        compiler_params=pltpu.CompilerParams(
            collective_id=0, has_side_effects=True, vmem_limit_bytes=56 * 1024 * 1024
        ),
    )(
        normed,
        pool_input,
        query_weight,
        key_weight,
        value_weight,
        pool_map,
        pool_scale.reshape(group_count, 1, GROUP_DIM),
        head_gain.reshape(1, 2 * HEAD_DIM),
        diff_lambda,
        out_pool,
        out_heads,
        cosine,
        sine,
    )
    return out[None]


def solution(mesh):
    placed = (
        P("fs", "sp", None),
        P(),
        P(("sp", "fs"), "tp"),
        P(("sp", "fs"), "tp"),
        P(("sp", "fs"), "tp"),
        P(("sp", "fs"), "tp"),
        P("tp", None, None),
        P("tp"),
        P(),
        P(),
        P("tp", ("sp", "fs")),
        P("tp", ("sp", "fs")),
    )
    shape = dict(mesh.shape)

    def body(tokens, *rest):
        head_count = rest[3].shape[1] // (2 * HEAD_DIM)
        group_count = rest[5].shape[0]
        fits = (
            shape["fs"] == 4
            and shape["tp"] == 2
            and shape["sp"] == head_count == group_count == 4
            and tokens.shape[0] == 1
        )
        return (fused if fits else local)(tokens, *rest)

    return jax.shard_map(
        body, mesh=mesh, in_specs=placed, out_specs=P("fs", "sp", "tp"), check_vma=False
    )
```

```python
import math

import jax
import jax.numpy as jnp
from jax import lax
from jax.experimental import pallas as pl
from jax.experimental.pallas import tpu as pltpu
from jax.sharding import PartitionSpec as P

HEAD_DIM = 128
GROUP_DIM = 256


THETA = 500000.0
HEAD_SCALE = 0.8
NORM_EPS = 1e-06
HEAD_EPS = 1e-05


def from_behind(value, axis, steps):
    count = lax.axis_size(axis)
    first, last = (max(0, -steps), min(count, count - steps))
    return lax.ppermute(value, axis, [(source, source + steps) for source in range(first, last)])


def rotate(tensor, positions):
    half = HEAD_DIM // 2
    freqs = 1.0 / THETA ** (jnp.arange(half, dtype=jnp.float32) * 2.0 / HEAD_DIM)
    angles = positions[:, None] * freqs[None, :]
    cosine = jnp.cos(angles)[:, None, None, :]
    sine = jnp.sin(angles)[:, None, None, :]
    floated = tensor.astype(jnp.float32)
    first = floated[..., :half]
    second = floated[..., half:]
    turned = jnp.concatenate([first * cosine - second * sine, second * cosine + first * sine], -1)
    return turned.astype(jnp.bfloat16)


def local(
    tokens,
    norm_gain,
    pool_input,
    query_weight,
    key_weight,
    value_weight,
    pool_map,
    pool_scale,
    head_gain,
    diff_lambda,
    out_pool,
    out_heads,
):
    out_local = jnp.concatenate([out_pool, out_heads], 0)
    row_count = tokens.shape[1]
    floated = tokens[0].astype(jnp.float32)
    normed = (
        floated * lax.rsqrt(jnp.mean(floated * floated, -1, keepdims=True) + NORM_EPS) * norm_gain
    ).astype(jnp.bfloat16)
    fragments = (
        lax.all_gather(pool_input, ("sp", "fs"), axis=0, tiled=True),
        lax.all_gather(query_weight, ("sp", "fs"), axis=0, tiled=True),
        lax.all_gather(key_weight, ("sp", "fs"), axis=0, tiled=True),
        lax.all_gather(value_weight, ("sp", "fs"), axis=0, tiled=True),
    )
    projected = tuple(
        (jnp.dot(normed, fragment, preferred_element_type=jnp.float32) for fragment in fragments)
    )
    pool_in, queries, keys_flat, values_flat = [
        product.astype(jnp.bfloat16) for product in projected
    ]
    head_count = values_flat.shape[1] // (2 * HEAD_DIM)
    tp_index = lax.axis_index("tp")
    sp_index = lax.axis_index("sp")
    query_pos = sp_index * row_count + jnp.arange(row_count, dtype=jnp.int32)
    positions = query_pos.astype(jnp.float32)
    queries = rotate(queries.reshape(row_count, head_count, 2, HEAD_DIM), positions)
    keys_flat = rotate(keys_flat.reshape(row_count, head_count, 2, HEAD_DIM), positions).reshape(
        row_count, head_count * 2 * HEAD_DIM
    )
    lambdas = lax.dynamic_slice_in_dim(diff_lambda, tp_index * head_count, head_count, 0)

    def online_step(state, key_rows, value_rows, key_offset):
        largest, summed, accum = state
        width = key_rows.shape[0]
        shaped = key_rows.reshape(width, head_count, 2, HEAD_DIM)
        scores = jnp.einsum(
            "qhcd,khcd->chqk", queries, shaped, preferred_element_type=jnp.float32
        ) * HEAD_DIM ** (-0.5)
        key_pos = key_offset + jnp.arange(width, dtype=jnp.int32)
        scores = jnp.where(query_pos[:, None] >= key_pos[None, :], scores, -jnp.inf)
        newest = jnp.maximum(largest, jnp.max(scores, -1))
        anchor = jnp.where(jnp.isfinite(newest), newest, 0.0)
        rescale = jnp.exp(largest - anchor)
        expons = jnp.exp(scores - anchor[..., None])
        summed = summed * rescale + jnp.sum(expons, -1)
        value_shaped = value_rows.reshape(width, head_count, 2 * HEAD_DIM)
        added = jnp.einsum(
            "chqk,khe->chqe",
            expons.astype(jnp.bfloat16),
            value_shaped,
            preferred_element_type=jnp.float32,
        )
        accum = accum * rescale[..., None] + added
        return (newest, summed, accum)

    start_state = (
        jnp.full((2, head_count, row_count), -jnp.inf, jnp.float32),
        jnp.zeros((2, head_count, row_count), jnp.float32),
        jnp.zeros((2, head_count, row_count, 2 * HEAD_DIM), jnp.float32),
    )
    fragments = (
        lax.all_gather(keys_flat, "sp", axis=0, tiled=True),
        lax.all_gather(values_flat, "sp", axis=0, tiled=True),
    )
    span = math.gcd(fragments[0].shape[0], 1024)

    def inner_step(index, inner_state):
        key_rows = lax.dynamic_slice_in_dim(fragments[0], index * span, span, 0)
        value_rows = lax.dynamic_slice_in_dim(fragments[1], index * span, span, 0)
        return online_step(inner_state, key_rows, value_rows, index * span)

    final_state = lax.fori_loop(0, fragments[0].shape[0] // span, inner_step, start_state)
    summed_final = final_state[1]
    accum_final = final_state[2]
    heads_raw = (
        accum_final[0] / summed_final[0][..., None]
        - lambdas[:, None, None] * accum_final[1] / summed_final[1][..., None]
    )
    heads_raw = jnp.moveaxis(heads_raw, 0, 1)
    attn = (
        (
            heads_raw
            * lax.rsqrt(jnp.mean(heads_raw * heads_raw, -1, keepdims=True) + HEAD_EPS)
            * head_gain
            * HEAD_SCALE
        )
        .astype(jnp.bfloat16)
        .reshape(row_count, head_count * 2 * HEAD_DIM)
    )
    reach = 15
    rim_rows = from_behind(pool_in[row_count - reach :], "sp", 1)
    extended = jnp.concatenate([rim_rows, pool_in], 0).astype(jnp.float32)
    pair_sums = extended[1:] + extended[:-1]
    quad_sums = pair_sums[2:] + pair_sums[:-2]
    octet_sums = quad_sums[4:] + quad_sums[:-4]
    sixteen_sums = octet_sums[8:] + octet_sums[:-8]
    group_count = pool_in.shape[1] // GROUP_DIM
    stacked = jnp.stack(
        [
            pair_sums[14 : 14 + row_count],
            quad_sums[12 : 12 + row_count],
            octet_sums[8 : 8 + row_count],
            sixteen_sums,
        ],
        0,
    ).reshape(4, row_count, group_count, GROUP_DIM)
    levels = (tp_index * group_count + jnp.arange(group_count, dtype=jnp.int32)) % 4
    picked = jnp.sum(
        jnp.where(
            levels[None, None, :, None] == jnp.arange(4, dtype=jnp.int32)[:, None, None, None],
            stacked,
            0.0,
        ),
        0,
    )
    windows = 2 ** (1 + levels)
    counts = jnp.minimum(query_pos[:, None] + 1, windows[None, :]).astype(jnp.float32)
    window_mean = picked / counts[:, :, None]
    grouped = pool_in.reshape(row_count, group_count, GROUP_DIM).astype(jnp.float32)
    pool_mixed = (window_mean - grouped).astype(jnp.bfloat16)
    pooled = (
        (
            jnp.einsum("tgc,gce->tge", pool_mixed, pool_map, preferred_element_type=jnp.float32)
            * pool_scale.reshape(group_count, GROUP_DIM)
        )
        .astype(jnp.bfloat16)
        .reshape(row_count, group_count * GROUP_DIM)
    )
    branches = jnp.concatenate([pooled, attn], 1)
    partial_value = jnp.dot(
        branches,
        lax.all_gather(out_local, ("sp", "fs"), axis=1, tiled=True),
        preferred_element_type=jnp.float32,
    )
    layer_out = lax.psum_scatter(
        partial_value.astype(jnp.bfloat16), "tp", scatter_dimension=1, tiled=True
    )
    return layer_out[None]


MESH = pl.DeviceIdType.MESH
PIECES = 2

def fused_kernel(
    places,
    groups,
    tokens_ref,
    norm_gain_ref,
    freqs_ref,
    pool_ref,
    query_ref,
    key_ref,
    value_ref,
    map_ref,
    scale_ref,
    gain_ref,
    lambda_ref,
    out_pool_ref,
    out_heads_ref,
    out_ref,
    normed_ref,
    cos_ref,
    sin_ref,
    rows_all,
    weights,
    outs,
    queries,
    keys,
    values,
    pools,
    to_mate,
    from_mate,
    to_peer,
    from_peer,
    merging,
    final,
    *sems,
):
    (
        own_sem,
        in_local,
        in_z_send,
        in_z_recv,
        in_n_send,
        in_n_recv,
        in_f_send,
        in_f_recv,
        out_local,
        out_z_send,
        out_z_recv,
        out_n_send,
        out_n_recv,
        out_f_send,
        out_f_recv,
        right_send,
        right_recv,
        left_send,
        left_recv,
        mate_send,
        mate_recv,
        half_send,
        half_recv,
        peer_send,
        peer_recv,
        merge_send,
        merge_recv,
    ) = sems
    z = lax.axis_index("sp")
    f = lax.axis_index("fs")
    c = lax.axis_index("tp")
    fx = f + 1 - 2 * lax.rem(f, 2)
    fy = lax.rem(f + 2, groups)
    mate = 1 - c
    half_rows = tokens_ref.shape[0] // 2
    row_count = 2 * half_rows
    depth = pool_ref.shape[0]
    width = GROUP_DIM
    out_width = out_pool_ref.shape[1]
    half_out = out_ref.shape[1]

    barrier = pltpu.get_barrier_semaphore()
    partners = [{"sp": lax.rem(z + d, places)} for d in range(1, places)]
    partners += [{"fs": fx}, {"fs": fy}, {"tp": mate}]
    for partner in partners:
        pl.semaphore_signal(barrier, inc=1, device_id=partner, device_id_type=MESH)
    pl.semaphore_wait(barrier, len(partners))

    def remote(source, target, send, recv, device):
        return pltpu.make_async_remote_copy(
            src_ref=source,
            dst_ref=target,
            send_sem=send,
            recv_sem=recv,
            device_id=device,
            device_id_type=MESH,
        )

    def block(index, size):
        return pl.ds(pl.multiple_of(index * size, size), size)

    class Gather:
        def __init__(self, sources, cut, view, group):
            self.sources, self.cut, self.view = sources, cut, view
            self.count = len(sources)
            (
                self.local,
                self.z_send,
                self.z_recv,
                self.n_send,
                self.n_recv,
                self.f_send,
                self.f_recv,
            ) = group
            self.low = (0, self.count // 2)
            self.high = (self.count // 2, self.count - self.count // 2)

        def own(self, m):
            return pltpu.make_async_copy(
                self.cut(self.sources[m], z), self.view(z, f, m, 1).at[0], self.local.at[m]
            )

        def across(self, d, m):
            to = lax.rem(z + d, places)
            return remote(
                self.cut(self.sources[m], to),
                self.view(z, f, m, 1).at[0],
                self.z_send.at[d, m],
                self.z_recv.at[d, m],
                {"sp": to},
            )

        def arrive(self, d, m):
            view = self.view(lax.rem(z + places - d, places), f, m, 1).at[0]
            return remote(
                view,
                view,
                self.z_send.at[d, m],
                self.z_recv.at[d, m],
                {"sp": lax.rem(z + places - d, places)},
            )

        def near(self, d, side, column):
            view = self.view(lax.rem(z + places - d, places), column, 0, self.count)
            return remote(
                view,
                view,
                self.n_send.at[side, d],
                self.n_recv.at[side, d],
                {"fs": (fx, fy)[side]},
            )

        def forward(self, d, side, column):
            start, size = (self.high, self.low)[side]
            view = self.view(lax.rem(z + places - d, places), column, start, size)
            return remote(
                view,
                view,
                self.f_send.at[side, d],
                self.f_recv.at[side, d],
                {"fs": (fx, fy)[side]},
            )

        def start(self):
            for m in range(self.count):
                self.own(m).start()
            for d in range(1, places):
                for m in range(self.count):
                    self.across(d, m).start()

        def first(self, d):
            for m in range(self.count):
                if d == 0:
                    self.own(m).wait()
                else:
                    self.arrive(d, m).wait_recv()
            for side in range(2):
                self.near(d, side, f).start()

        def second(self, d):
            self.near(d, 0, fx).wait_recv()
            self.forward(d, 1, fx).start()
            self.near(d, 1, fy).wait_recv()
            self.forward(d, 0, fy).start()

        def third(self, d):
            diagonal = lax.rem(fx + 2, groups)
            for side in range(2):
                self.forward(d, side, diagonal).wait_recv()

        def drain(self):
            for d in range(places):
                for m in range(self.count):
                    if d > 0:
                        self.across(d, m).wait_send()
                for side in range(2):
                    self.near(d, side, f).wait_send()
                self.forward(d, 1, fx).wait_send()
                self.forward(d, 0, fy).wait_send()

    inward = Gather(
        (pool_ref, query_ref, key_ref, value_ref),
        lambda ref, to: ref.at[:, block(to, width)],
        lambda zz, ff, m, n: weights.at[pl.ds(m, n), block(zz * groups + ff, depth), :],
        (in_local, in_z_send, in_z_recv, in_n_send, in_n_recv, in_f_send, in_f_recv),
    )
    outward = Gather(
        (out_pool_ref, out_heads_ref),
        lambda ref, to: ref.at[block(to, width), :],
        lambda zz, ff, m, n: outs.at[pl.ds(m, n), :, block(zz * groups + ff, out_width)],
        (out_local, out_z_send, out_z_recv, out_n_send, out_n_recv, out_f_send, out_f_recv),
    )

    piece_rows = half_rows // PIECES

    def chunk(zz, side, p):
        return rows_all.at[block((2 * zz + side) * PIECES + p, piece_rows), :]

    def right(k, p):
        view = chunk(z - k, c, p)
        return remote(view, view, right_send.at[k, p], right_recv.at[k + 1, p], {"sp": z + 1})

    def from_left(k, p):
        view = chunk(z - k, c, p)
        return remote(view, view, right_send.at[k, p], right_recv.at[k, p], {"sp": z - 1})

    def left(k, p):
        view = chunk(z + k, c, p)
        return remote(view, view, left_send.at[k, p], left_recv.at[k + 1, p], {"sp": z - 1})

    def from_right(k, p):
        view = chunk(z + k, c, p)
        return remote(view, view, left_send.at[k, p], left_recv.at[k, p], {"sp": z + 1})

    def share(slot, zz, side, p):
        view = chunk(zz, side, p)
        return remote(view, view, mate_send.at[slot, p], mate_recv.at[slot, p], {"tp": mate})

    own_rows = pltpu.make_async_copy(
        normed_ref, rows_all.at[block(2 * z + c, half_rows), :], own_sem
    )
    inward.start()
    outward.start()
    floated = tokens_ref[pl.ds(pl.multiple_of(c * half_rows, 16), half_rows), :].astype(
        jnp.float32
    )
    normed_ref[...] = (
        floated
        * lax.rsqrt(jnp.mean(floated * floated, -1, keepdims=True) + NORM_EPS)
        * norm_gain_ref[...]
    ).astype(jnp.bfloat16)
    own_rows.start()
    own_rows.wait()

    @pl.when(z < places - 1)
    def _():
        for p in range(PIECES):
            right(0, p).start()

    @pl.when(z > 0)
    def _():
        for p in range(PIECES):
            left(0, p).start()

    for p in range(PIECES):
        share(0, z, c, p).start()

    def tokens_step(k):
        for p in range(PIECES):

            @pl.when(z >= k)
            def _():
                from_left(k, p).wait_recv()

                @pl.when(z < places - 1)
                def _():
                    right(k, p).start()

                share(k, z - k, c, p).start()

            @pl.when(z + k < places)
            def _():
                from_right(k, p).wait_recv()

                @pl.when(z > 0)
                def _():
                    left(k, p).start()

                share(places - 1 + k, z + k, c, p).start()

    pools[0:16, :] = jnp.zeros((16, width), jnp.bfloat16)
    inward.first(0)

    def table(index, carry):
        rows = block(index, row_count)
        half = HEAD_DIM // 2
        count = (
            index * row_count + lax.broadcasted_iota(jnp.int32, (row_count, HEAD_DIM), 0)
        ).astype(jnp.float32)
        lane = lax.broadcasted_iota(jnp.int32, (row_count, HEAD_DIM), 1)
        angles = count * freqs_ref[...]
        cos_ref[rows, :] = jnp.cos(angles)
        sine = jnp.sin(angles)
        sin_ref[rows, :] = jnp.where(lane < half, -sine, sine)
        return carry

    lax.fori_loop(0, places, table, 0)
    for d in range(1, places):
        inward.first(d)
        inward.second(d - 1)
    outward.first(0)
    inward.second(places - 1)
    for d in range(1, places):
        outward.first(d)
        if d > 1:
            outward.second(d - 2)
    tokens_step(1)
    for d in (places - 2, places - 1):
        outward.second(d)
    for k in range(2, places):
        tokens_step(k)
    for d in range(places):
        inward.third(d)

    for p in range(PIECES):
        share(0, z, mate, p).wait_recv()
        for k in range(1, places):

            @pl.when(z >= k)
            def _():
                share(k, z - k, mate, p).wait_recv()

            @pl.when(z + k < places)
            def _():
                share(places - 1 + k, z + k, mate, p).wait_recv()

    def turned(raw, cosine, sine):
        floated = raw.astype(jnp.float32)
        return (floated * cosine + pltpu.roll(floated, HEAD_DIM // 2, 1) * sine).astype(
            jnp.bfloat16
        )

    def project(index, carry):
        rows = block(index, row_count)
        normed = rows_all[rows, :]
        cosine = cos_ref[rows, :]
        sine = sin_ref[rows, :]

        def product(m):
            return jnp.dot(normed, weights[m], preferred_element_type=jnp.float32).astype(
                jnp.bfloat16
            )

        pools[pl.ds(pl.multiple_of(index * row_count + 16, 16), row_count), :] = product(0)
        raw = product(1)
        for m in range(2):
            part = slice(m * HEAD_DIM, (m + 1) * HEAD_DIM)
            queries[rows, part] = turned(raw[:, part], cosine, sine)
        raw = product(2)
        for m in range(2):
            part = slice(m * HEAD_DIM, (m + 1) * HEAD_DIM)
            keys[rows, part] = turned(raw[:, part], cosine, sine)
        values[rows, :] = product(3)
        return carry

    lax.fori_loop(0, places, project, 0)
    for d in range(places):
        outward.third(d)

    level = lax.rem(c * map_ref.shape[0] + z, 4)
    window = jnp.where(
        level == 0, 2, jnp.where(level == 1, 4, jnp.where(level == 2, 8, 16))
    )
    head_lambda = lambda_ref[c * map_ref.shape[0] + z]
    length = places * row_count

    def to_sibling(d, to):
        return remote(
            to_mate.at[to], from_mate.at[to], half_send.at[d], half_recv.at[d], {"tp": mate}
        )

    outer = (z == 0) | (z == places - 1)
    pair = z + 1 - 2 * lax.rem(z, 2)
    far = jnp.where(z < 2, places - 1, 0)
    near = jnp.where(z < 2, 2, 1)

    def to_inner(role, to):
        return remote(
            to_peer.at[to], merging.at[role], merge_send.at[role], merge_recv.at[role], {"sp": pair}
        )

    def to_place(role, to):
        return remote(
            to_peer.at[to], from_peer.at[0], peer_send.at[role], peer_recv.at[0], {"sp": to}
        )

    def to_pair():
        return remote(
            to_peer.at[pair], from_peer.at[1], peer_send.at[2], peer_recv.at[1], {"sp": pair}
        )

    def compute(step, carry):
        role = jnp.where((step == 3) | outer, step, lax.rem(step + 2, 3))
        to = jnp.where(role == 0, far, jnp.where(role == 1, near, jnp.where(role == 2, pair, z)))
        d = step
        rows = block(to, row_count)
        query_pos = to * row_count + lax.broadcasted_iota(jnp.int32, (row_count, length), 0)
        key_pos = lax.broadcasted_iota(jnp.int32, (row_count, length), 1)
        seen = query_pos >= key_pos
        mapped = []
        for m in range(2):
            part = slice(m * HEAD_DIM, (m + 1) * HEAD_DIM)
            scores = lax.dot_general(
                queries[rows, part],
                keys[:, part],
                (((1,), (1,)), ((), ())),
                preferred_element_type=jnp.float32,
            ) * HEAD_DIM ** (-0.5)
            scores = jnp.where(seen, scores, -jnp.inf)
            expons = jnp.exp(scores - jnp.max(scores, -1, keepdims=True))
            totals = jnp.sum(expons, -1, keepdims=True)
            mapped.append(
                jnp.dot(
                    expons.astype(jnp.bfloat16), values[...], preferred_element_type=jnp.float32
                )
                / totals
            )
        raw = mapped[0] - head_lambda * mapped[1]
        attn = (
            raw
            * lax.rsqrt(jnp.mean(raw * raw, -1, keepdims=True) + HEAD_EPS)
            * gain_ref[...]
            * HEAD_SCALE
        ).astype(jnp.bfloat16)
        extended = pools[
            pl.ds(pl.multiple_of(to * row_count, 16), row_count + 16), :
        ].astype(jnp.float32)
        picked = extended + pltpu.roll(extended, 1, 0)
        sums = picked
        for shift in (2, 4, 8):
            sums = sums + pltpu.roll(sums, shift, 0)
            picked = lax.select_n(window >= 2 * shift, picked, sums)
        places_of = to * row_count + lax.broadcasted_iota(jnp.int32, (row_count, 1), 0)
        counts = jnp.minimum(places_of + 1, window).astype(jnp.float32)
        mixed = (picked[16:] / counts - extended[16:]).astype(jnp.bfloat16)
        pooled = (
            jnp.dot(mixed, map_ref[z], preferred_element_type=jnp.float32) * scale_ref[z]
        ).astype(jnp.bfloat16)

        def partial_of(side):
            columns = block(side, half_out)
            return jnp.dot(
                pooled, outs[0, :, columns], preferred_element_type=jnp.float32
            ) + jnp.dot(attn, outs[1, :, columns], preferred_element_type=jnp.float32)

        to_mate[to] = partial_of(mate).astype(jnp.bfloat16)
        to_sibling(d, to).start()
        mine = partial_of(c)
        to_sibling(d, to).wait_recv()
        summed = mine + from_mate[to].astype(jnp.float32)

        @pl.when((role < 2) & outer)
        def _():
            to_peer[to] = summed.astype(jnp.bfloat16)
            to_inner(role, to).start()

        @pl.when((role < 2) & jnp.logical_not(outer))
        def _():
            to_inner(role, to).wait_recv()
            to_peer[to] = (summed + merging[role].astype(jnp.float32)).astype(jnp.bfloat16)
            to_place(role, to).start()

        @pl.when(role == 2)
        def _():
            to_peer[to] = summed.astype(jnp.bfloat16)
            to_pair().start()

        @pl.when(role == 3)
        def _():
            final[...] = summed

        return carry

    lax.fori_loop(0, places, compute, 0)

    to_pair().wait_recv()
    total = final[...] + from_peer[1].astype(jnp.float32)
    to_place(0, z).wait_recv()
    out_ref[...] = (total + from_peer[0].astype(jnp.float32)).astype(out_ref.dtype)

    inward.drain()
    outward.drain()

    for p in range(PIECES):

        @pl.when(z < places - 1)
        def _():
            right(0, p).wait_send()

        @pl.when(z > 0)
        def _():
            left(0, p).wait_send()

        share(0, z, c, p).wait_send()
        for k in range(1, places):

            @pl.when(z >= k)
            def _():
                @pl.when(z < places - 1)
                def _():
                    right(k, p).wait_send()

                share(k, z - k, c, p).wait_send()

            @pl.when(z + k < places)
            def _():
                @pl.when(z > 0)
                def _():
                    left(k, p).wait_send()

                share(places - 1 + k, z + k, c, p).wait_send()

    for d in range(places):
        to_sibling(d, d).wait_send()
    for role, to in ((0, far), (1, near)):

        @pl.when(outer)
        def _():
            to_inner(role, to).wait_send()

        @pl.when(jnp.logical_not(outer))
        def _():
            to_place(role, to).wait_send()

    to_pair().wait_send()


def fused(
    tokens,
    norm_gain,
    pool_input,
    query_weight,
    key_weight,
    value_weight,
    pool_map,
    pool_scale,
    head_gain,
    diff_lambda,
    out_pool,
    out_heads,
):
    places = lax.axis_size("sp")
    groups = lax.axis_size("fs")
    row_count, model = tokens.shape[1], tokens.shape[2]
    length = places * row_count
    half = HEAD_DIM // 2
    freqs = 1.0 / THETA ** (jnp.arange(half, dtype=jnp.float32) * 2.0 / HEAD_DIM)
    freqs = jnp.concatenate([freqs, freqs])[None, :]
    group_count = pool_map.shape[0]
    half_out = model // 2
    vmem = pl.BlockSpec(memory_space=pltpu.VMEM)
    smem = pl.BlockSpec(memory_space=pltpu.SMEM)
    dma = pltpu.SemaphoreType.DMA
    low = jnp.bfloat16

    def gather_sems(count):
        return [
            dma((count,)),
            dma((places, count)),
            dma((places, count)),
            dma((2, places)),
            dma((2, places)),
            dma((2, places)),
            dma((2, places)),
        ]

    out = pl.pallas_call(
        lambda *refs: fused_kernel(places, groups, *refs),
        out_shape=jax.ShapeDtypeStruct((row_count, half_out), low),
        in_specs=[vmem] * 10 + [smem] + [vmem] * 2,
        out_specs=vmem,
        scratch_shapes=[
            pltpu.VMEM((row_count // 2, model), low),
            pltpu.VMEM((length, HEAD_DIM), jnp.float32),
            pltpu.VMEM((length, HEAD_DIM), jnp.float32),
            pltpu.VMEM((length, model), low),
            pltpu.VMEM((4, model, GROUP_DIM), low),
            pltpu.VMEM((2, GROUP_DIM, model), low),
            pltpu.VMEM((length, GROUP_DIM), low),
            pltpu.VMEM((length, GROUP_DIM), low),
            pltpu.VMEM((length, GROUP_DIM), low),
            pltpu.VMEM((length + 16, GROUP_DIM), low),
            pltpu.VMEM((places, row_count, half_out), low),
            pltpu.VMEM((places, row_count, half_out), low),
            pltpu.VMEM((places, row_count, half_out), low),
            pltpu.VMEM((2, row_count, half_out), low),
            pltpu.VMEM((2, row_count, half_out), low),
            pltpu.VMEM((row_count, half_out), jnp.float32),
            dma,
            *gather_sems(4),
            *gather_sems(2),
            dma((places, PIECES)),
            dma((places + 1, PIECES)),
            dma((places, PIECES)),
            dma((places + 1, PIECES)),
            dma((2 * places, PIECES)),
            dma((2 * places, PIECES)),
            dma((places,)),
            dma((places,)),
            dma((3,)),
            dma((2,)),
            dma((2,)),
            dma((2,)),
        ],
        compiler_params=pltpu.CompilerParams(
            collective_id=0, has_side_effects=True, vmem_limit_bytes=56 * 1024 * 1024
        ),
    )(
        tokens[0],
        norm_gain.reshape(1, model),
        freqs,
        pool_input,
        query_weight,
        key_weight,
        value_weight,
        pool_map,
        pool_scale.reshape(group_count, 1, GROUP_DIM),
        head_gain.reshape(1, 2 * HEAD_DIM),
        diff_lambda,
        out_pool,
        out_heads,
    )
    return out[None]


def solution(mesh):
    placed = (
        P("fs", "sp", None),
        P(),
        P(("sp", "fs"), "tp"),
        P(("sp", "fs"), "tp"),
        P(("sp", "fs"), "tp"),
        P(("sp", "fs"), "tp"),
        P("tp", None, None),
        P("tp"),
        P(),
        P(),
        P("tp", ("sp", "fs")),
        P("tp", ("sp", "fs")),
    )
    shape = dict(mesh.shape)

    def body(tokens, *rest):
        head_count = rest[3].shape[1] // (2 * HEAD_DIM)
        group_count = rest[5].shape[0]
        fits = (
            shape["fs"] == 4
            and shape["tp"] == 2
            and shape["sp"] == head_count == group_count == 4
            and tokens.shape[0] == 1
        )
        return (fused if fits else local)(tokens, *rest)

    return jax.shard_map(
        body, mesh=mesh, in_specs=placed, out_specs=P("fs", "sp", "tp"), check_vma=False
    )
```

```python
import math

import jax
import jax.numpy as jnp
from jax import lax
from jax.experimental import pallas as pl
from jax.experimental.pallas import tpu as pltpu
from jax.sharding import PartitionSpec as P

HEAD_DIM = 128
GROUP_DIM = 256


THETA = 500000.0
HEAD_SCALE = 0.8
NORM_EPS = 1e-06
HEAD_EPS = 1e-05


def from_behind(value, axis, steps):
    count = lax.axis_size(axis)
    first, last = (max(0, -steps), min(count, count - steps))
    return lax.ppermute(value, axis, [(source, source + steps) for source in range(first, last)])


def rotate(tensor, positions):
    half = HEAD_DIM // 2
    freqs = 1.0 / THETA ** (jnp.arange(half, dtype=jnp.float32) * 2.0 / HEAD_DIM)
    angles = positions[:, None] * freqs[None, :]
    cosine = jnp.cos(angles)[:, None, None, :]
    sine = jnp.sin(angles)[:, None, None, :]
    floated = tensor.astype(jnp.float32)
    first = floated[..., :half]
    second = floated[..., half:]
    turned = jnp.concatenate([first * cosine - second * sine, second * cosine + first * sine], -1)
    return turned.astype(jnp.bfloat16)


def local(
    tokens,
    norm_gain,
    pool_input,
    query_weight,
    key_weight,
    value_weight,
    pool_map,
    pool_scale,
    head_gain,
    diff_lambda,
    out_pool,
    out_heads,
):
    out_local = jnp.concatenate([out_pool, out_heads], 0)
    row_count = tokens.shape[1]
    floated = tokens[0].astype(jnp.float32)
    normed = (
        floated * lax.rsqrt(jnp.mean(floated * floated, -1, keepdims=True) + NORM_EPS) * norm_gain
    ).astype(jnp.bfloat16)
    fragments = (
        lax.all_gather(pool_input, ("sp", "fs"), axis=0, tiled=True),
        lax.all_gather(query_weight, ("sp", "fs"), axis=0, tiled=True),
        lax.all_gather(key_weight, ("sp", "fs"), axis=0, tiled=True),
        lax.all_gather(value_weight, ("sp", "fs"), axis=0, tiled=True),
    )
    projected = tuple(
        (jnp.dot(normed, fragment, preferred_element_type=jnp.float32) for fragment in fragments)
    )
    pool_in, queries, keys_flat, values_flat = [
        product.astype(jnp.bfloat16) for product in projected
    ]
    head_count = values_flat.shape[1] // (2 * HEAD_DIM)
    tp_index = lax.axis_index("tp")
    sp_index = lax.axis_index("sp")
    query_pos = sp_index * row_count + jnp.arange(row_count, dtype=jnp.int32)
    positions = query_pos.astype(jnp.float32)
    queries = rotate(queries.reshape(row_count, head_count, 2, HEAD_DIM), positions)
    keys_flat = rotate(keys_flat.reshape(row_count, head_count, 2, HEAD_DIM), positions).reshape(
        row_count, head_count * 2 * HEAD_DIM
    )
    lambdas = lax.dynamic_slice_in_dim(diff_lambda, tp_index * head_count, head_count, 0)

    def online_step(state, key_rows, value_rows, key_offset):
        largest, summed, accum = state
        width = key_rows.shape[0]
        shaped = key_rows.reshape(width, head_count, 2, HEAD_DIM)
        scores = jnp.einsum(
            "qhcd,khcd->chqk", queries, shaped, preferred_element_type=jnp.float32
        ) * HEAD_DIM ** (-0.5)
        key_pos = key_offset + jnp.arange(width, dtype=jnp.int32)
        scores = jnp.where(query_pos[:, None] >= key_pos[None, :], scores, -jnp.inf)
        newest = jnp.maximum(largest, jnp.max(scores, -1))
        anchor = jnp.where(jnp.isfinite(newest), newest, 0.0)
        rescale = jnp.exp(largest - anchor)
        expons = jnp.exp(scores - anchor[..., None])
        summed = summed * rescale + jnp.sum(expons, -1)
        value_shaped = value_rows.reshape(width, head_count, 2 * HEAD_DIM)
        added = jnp.einsum(
            "chqk,khe->chqe",
            expons.astype(jnp.bfloat16),
            value_shaped,
            preferred_element_type=jnp.float32,
        )
        accum = accum * rescale[..., None] + added
        return (newest, summed, accum)

    start_state = (
        jnp.full((2, head_count, row_count), -jnp.inf, jnp.float32),
        jnp.zeros((2, head_count, row_count), jnp.float32),
        jnp.zeros((2, head_count, row_count, 2 * HEAD_DIM), jnp.float32),
    )
    fragments = (
        lax.all_gather(keys_flat, "sp", axis=0, tiled=True),
        lax.all_gather(values_flat, "sp", axis=0, tiled=True),
    )
    span = math.gcd(fragments[0].shape[0], 1024)

    def inner_step(index, inner_state):
        key_rows = lax.dynamic_slice_in_dim(fragments[0], index * span, span, 0)
        value_rows = lax.dynamic_slice_in_dim(fragments[1], index * span, span, 0)
        return online_step(inner_state, key_rows, value_rows, index * span)

    final_state = lax.fori_loop(0, fragments[0].shape[0] // span, inner_step, start_state)
    summed_final = final_state[1]
    accum_final = final_state[2]
    heads_raw = (
        accum_final[0] / summed_final[0][..., None]
        - lambdas[:, None, None] * accum_final[1] / summed_final[1][..., None]
    )
    heads_raw = jnp.moveaxis(heads_raw, 0, 1)
    attn = (
        (
            heads_raw
            * lax.rsqrt(jnp.mean(heads_raw * heads_raw, -1, keepdims=True) + HEAD_EPS)
            * head_gain
            * HEAD_SCALE
        )
        .astype(jnp.bfloat16)
        .reshape(row_count, head_count * 2 * HEAD_DIM)
    )
    reach = 15
    rim_rows = from_behind(pool_in[row_count - reach :], "sp", 1)
    extended = jnp.concatenate([rim_rows, pool_in], 0).astype(jnp.float32)
    pair_sums = extended[1:] + extended[:-1]
    quad_sums = pair_sums[2:] + pair_sums[:-2]
    octet_sums = quad_sums[4:] + quad_sums[:-4]
    sixteen_sums = octet_sums[8:] + octet_sums[:-8]
    group_count = pool_in.shape[1] // GROUP_DIM
    stacked = jnp.stack(
        [
            pair_sums[14 : 14 + row_count],
            quad_sums[12 : 12 + row_count],
            octet_sums[8 : 8 + row_count],
            sixteen_sums,
        ],
        0,
    ).reshape(4, row_count, group_count, GROUP_DIM)
    levels = (tp_index * group_count + jnp.arange(group_count, dtype=jnp.int32)) % 4
    picked = jnp.sum(
        jnp.where(
            levels[None, None, :, None] == jnp.arange(4, dtype=jnp.int32)[:, None, None, None],
            stacked,
            0.0,
        ),
        0,
    )
    windows = 2 ** (1 + levels)
    counts = jnp.minimum(query_pos[:, None] + 1, windows[None, :]).astype(jnp.float32)
    window_mean = picked / counts[:, :, None]
    grouped = pool_in.reshape(row_count, group_count, GROUP_DIM).astype(jnp.float32)
    pool_mixed = (window_mean - grouped).astype(jnp.bfloat16)
    pooled = (
        (
            jnp.einsum("tgc,gce->tge", pool_mixed, pool_map, preferred_element_type=jnp.float32)
            * pool_scale.reshape(group_count, GROUP_DIM)
        )
        .astype(jnp.bfloat16)
        .reshape(row_count, group_count * GROUP_DIM)
    )
    branches = jnp.concatenate([pooled, attn], 1)
    partial_value = jnp.dot(
        branches,
        lax.all_gather(out_local, ("sp", "fs"), axis=1, tiled=True),
        preferred_element_type=jnp.float32,
    )
    layer_out = lax.psum_scatter(
        partial_value.astype(jnp.bfloat16), "tp", scatter_dimension=1, tiled=True
    )
    return layer_out[None]


MESH = pl.DeviceIdType.MESH
PIECES = 4
PARTS = 2

def fused_kernel(
    places,
    groups,
    tokens_ref,
    norm_gain_ref,
    freqs_ref,
    pool_ref,
    query_ref,
    key_ref,
    value_ref,
    map_ref,
    scale_ref,
    gain_ref,
    lambda_ref,
    out_pool_ref,
    out_heads_ref,
    out_ref,
    normed_ref,
    cos_ref,
    sin_ref,
    rows_all,
    weights,
    outs,
    queries,
    keys,
    values,
    pools,
    to_mate,
    from_mate,
    to_peer,
    from_peer,
    merging,
    final,
    *sems,
):
    (
        own_sem,
        in_local,
        in_z_send,
        in_z_recv,
        in_n_send,
        in_n_recv,
        in_f_send,
        in_f_recv,
        out_local,
        out_z_send,
        out_z_recv,
        out_n_send,
        out_n_recv,
        out_f_send,
        out_f_recv,
        right_send,
        right_recv,
        left_send,
        left_recv,
        mate_send,
        mate_recv,
        half_send,
        half_recv,
        peer_send,
        peer_recv,
        merge_send,
        merge_recv,
    ) = sems
    z = lax.axis_index("sp")
    f = lax.axis_index("fs")
    c = lax.axis_index("tp")
    fx = f + 1 - 2 * lax.rem(f, 2)
    fy = lax.rem(f + 2, groups)
    mate = 1 - c
    half_rows = tokens_ref.shape[0] // 2
    row_count = 2 * half_rows
    depth = pool_ref.shape[0]
    width = GROUP_DIM
    out_width = out_pool_ref.shape[1]
    half_out = out_ref.shape[1]

    barrier = pltpu.get_barrier_semaphore()
    partners = [{"sp": lax.rem(z + d, places)} for d in range(1, places)]
    partners += [{"fs": fx}, {"fs": fy}, {"tp": mate}]
    for partner in partners:
        pl.semaphore_signal(barrier, inc=1, device_id=partner, device_id_type=MESH)
    pl.semaphore_wait(barrier, len(partners))

    def remote(source, target, send, recv, device):
        return pltpu.make_async_remote_copy(
            src_ref=source,
            dst_ref=target,
            send_sem=send,
            recv_sem=recv,
            device_id=device,
            device_id_type=MESH,
        )

    def block(index, size):
        return pl.ds(pl.multiple_of(index * size, size), size)

    class Gather:
        def __init__(self, sources, cut, view, group):
            self.sources, self.cut, self.view = sources, cut, view
            self.count = len(sources)
            (
                self.local,
                self.z_send,
                self.z_recv,
                self.n_send,
                self.n_recv,
                self.f_send,
                self.f_recv,
            ) = group
            self.low = (0, self.count // 2)
            self.high = (self.count // 2, self.count - self.count // 2)

        def own(self, m):
            return pltpu.make_async_copy(
                self.cut(self.sources[m], z), self.view(z, f, m, 1).at[0], self.local.at[m]
            )

        def across(self, d, m):
            to = lax.rem(z + d, places)
            return remote(
                self.cut(self.sources[m], to),
                self.view(z, f, m, 1).at[0],
                self.z_send.at[d, m],
                self.z_recv.at[d, m],
                {"sp": to},
            )

        def arrive(self, d, m):
            view = self.view(lax.rem(z + places - d, places), f, m, 1).at[0]
            return remote(
                view,
                view,
                self.z_send.at[d, m],
                self.z_recv.at[d, m],
                {"sp": lax.rem(z + places - d, places)},
            )

        def near(self, d, side, column, half):
            start, size = (self.low, self.high)[half]
            view = self.view(lax.rem(z + places - d, places), column, start, size)
            return remote(
                view,
                view,
                self.n_send.at[side, 2 * d + half],
                self.n_recv.at[side, 2 * d + half],
                {"fs": (fx, fy)[side]},
            )

        def forward(self, d, side, column):
            start, size = (self.high, self.low)[side]
            view = self.view(lax.rem(z + places - d, places), column, start, size)
            return remote(
                view,
                view,
                self.f_send.at[side, d],
                self.f_recv.at[side, d],
                {"fs": (fx, fy)[side]},
            )

        def start(self):
            for m in range(self.count):
                self.own(m).start()
            for d in range(1, places):
                for m in range(self.count):
                    self.across(d, m).start()

        def first(self, d):
            for m in range(self.count):
                if d == 0:
                    self.own(m).wait()
                else:
                    self.arrive(d, m).wait_recv()
            for order in range(2):
                for side in range(2):
                    self.near(d, side, f, side ^ order).start()

        def second(self, d):
            self.near(d, 0, fx, 0).wait_recv()
            self.forward(d, 1, fx).start()
            self.near(d, 1, fy, 1).wait_recv()
            self.forward(d, 0, fy).start()

        def third(self, d):
            diagonal = lax.rem(fx + 2, groups)
            for side in range(2):
                self.forward(d, side, diagonal).wait_recv()
            self.near(d, 0, fx, 1).wait_recv()
            self.near(d, 1, fy, 0).wait_recv()

        def drain(self):
            for d in range(places):
                for m in range(self.count):
                    if d > 0:
                        self.across(d, m).wait_send()
                for side in range(2):
                    for half in range(2):
                        self.near(d, side, f, half).wait_send()
                self.forward(d, 1, fx).wait_send()
                self.forward(d, 0, fy).wait_send()

    inward = Gather(
        (pool_ref, query_ref, key_ref, value_ref),
        lambda ref, to: ref.at[:, block(to, width)],
        lambda zz, ff, m, n: weights.at[pl.ds(m, n), block(zz * groups + ff, depth), :],
        (in_local, in_z_send, in_z_recv, in_n_send, in_n_recv, in_f_send, in_f_recv),
    )
    outward = Gather(
        (out_pool_ref, out_heads_ref),
        lambda ref, to: ref.at[block(to, width), :],
        lambda zz, ff, m, n: outs.at[pl.ds(m, n), :, block(zz * groups + ff, out_width)],
        (out_local, out_z_send, out_z_recv, out_n_send, out_n_recv, out_f_send, out_f_recv),
    )

    piece_rows = half_rows // PIECES

    def chunk(zz, side, p):
        return rows_all.at[block((2 * zz + side) * PIECES + p, piece_rows), :]

    def right(k, p):
        view = chunk(z - k, c, p)
        return remote(view, view, right_send.at[k, p], right_recv.at[k + 1, p], {"sp": z + 1})

    def from_left(k, p):
        view = chunk(z - k, c, p)
        return remote(view, view, right_send.at[k, p], right_recv.at[k, p], {"sp": z - 1})

    def left(k, p):
        view = chunk(z + k, c, p)
        return remote(view, view, left_send.at[k, p], left_recv.at[k + 1, p], {"sp": z - 1})

    def from_right(k, p):
        view = chunk(z + k, c, p)
        return remote(view, view, left_send.at[k, p], left_recv.at[k, p], {"sp": z + 1})

    def share(slot, zz, side, p):
        view = chunk(zz, side, p)
        return remote(view, view, mate_send.at[slot, p], mate_recv.at[slot, p], {"tp": mate})

    own_rows = pltpu.make_async_copy(
        normed_ref, rows_all.at[block(2 * z + c, half_rows), :], own_sem
    )
    inward.start()
    outward.start()
    floated = tokens_ref[pl.ds(pl.multiple_of(c * half_rows, 16), half_rows), :].astype(
        jnp.float32
    )
    normed_ref[...] = (
        floated
        * lax.rsqrt(jnp.mean(floated * floated, -1, keepdims=True) + NORM_EPS)
        * norm_gain_ref[...]
    ).astype(jnp.bfloat16)
    own_rows.start()
    own_rows.wait()

    @pl.when(z < places - 1)
    def _():
        for p in range(PIECES):
            right(0, p).start()

    @pl.when(z > 0)
    def _():
        for p in range(PIECES):
            left(0, p).start()

    for p in range(PIECES):
        share(0, z, c, p).start()

    def tokens_step(k):
        for p in range(PIECES):

            @pl.when(z >= k)
            def _():
                from_left(k, p).wait_recv()

                @pl.when(z < places - 1)
                def _():
                    right(k, p).start()

                share(k, z - k, c, p).start()

            @pl.when(z + k < places)
            def _():
                from_right(k, p).wait_recv()

                @pl.when(z > 0)
                def _():
                    left(k, p).start()

                share(places - 1 + k, z + k, c, p).start()

    pools[0:16, :] = jnp.zeros((16, width), jnp.bfloat16)
    inward.first(0)

    def table(index, carry):
        rows = block(index, row_count)
        half = HEAD_DIM // 2
        count = (
            index * row_count + lax.broadcasted_iota(jnp.int32, (row_count, HEAD_DIM), 0)
        ).astype(jnp.float32)
        lane = lax.broadcasted_iota(jnp.int32, (row_count, HEAD_DIM), 1)
        angles = count * freqs_ref[...]
        cos_ref[rows, :] = jnp.cos(angles)
        sine = jnp.sin(angles)
        sin_ref[rows, :] = jnp.where(lane < half, -sine, sine)
        return carry

    lax.fori_loop(0, places, table, 0)
    for d in range(1, places):
        inward.first(d)
        inward.second(d - 1)
    outward.first(0)
    inward.second(places - 1)
    for d in range(1, places):
        outward.first(d)
        if d > 1:
            outward.second(d - 2)
    tokens_step(1)
    for d in (places - 2, places - 1):
        outward.second(d)
    for k in range(2, places):
        tokens_step(k)
    for d in range(places):
        inward.third(d)

    for p in range(PIECES):
        share(0, z, mate, p).wait_recv()
        for k in range(1, places):

            @pl.when(z >= k)
            def _():
                share(k, z - k, mate, p).wait_recv()

            @pl.when(z + k < places)
            def _():
                share(places - 1 + k, z + k, mate, p).wait_recv()

    def turned(raw, cosine, sine):
        floated = raw.astype(jnp.float32)
        return (floated * cosine + pltpu.roll(floated, HEAD_DIM // 2, 1) * sine).astype(
            jnp.bfloat16
        )

    def project(index, carry):
        rows = block(index, row_count)
        normed = rows_all[rows, :]
        cosine = cos_ref[rows, :]
        sine = sin_ref[rows, :]

        def product(m):
            return jnp.dot(normed, weights[m], preferred_element_type=jnp.float32).astype(
                jnp.bfloat16
            )

        pools[pl.ds(pl.multiple_of(index * row_count + 16, 16), row_count), :] = product(0)
        raw = product(1)
        for m in range(2):
            part = slice(m * HEAD_DIM, (m + 1) * HEAD_DIM)
            queries[rows, part] = turned(raw[:, part], cosine, sine)
        raw = product(2)
        for m in range(2):
            part = slice(m * HEAD_DIM, (m + 1) * HEAD_DIM)
            keys[rows, part] = turned(raw[:, part], cosine, sine)
        values[rows, :] = product(3)
        return carry

    lax.fori_loop(0, places, project, 0)
    for d in range(places):
        outward.third(d)

    level = lax.rem(c * map_ref.shape[0] + z, 4)
    window = jnp.where(
        level == 0, 2, jnp.where(level == 1, 4, jnp.where(level == 2, 8, 16))
    )
    head_lambda = lambda_ref[c * map_ref.shape[0] + z]
    length = places * row_count

    part_rows = row_count // PARTS

    def to_sibling(step):
        return remote(
            to_mate.at[step],
            from_mate.at[step],
            half_send.at[step],
            half_recv.at[step],
            {"tp": mate},
        )

    outer = (z == 0) | (z == places - 1)
    pair = z + 1 - 2 * lax.rem(z, 2)
    far = jnp.where(z < 2, places - 1, 0)
    near = jnp.where(z < 2, 2, 1)

    def to_inner(role, to, h):
        return remote(
            to_peer.at[to * PARTS + h],
            merging.at[role * PARTS + h],
            merge_send.at[role * PARTS + h],
            merge_recv.at[role * PARTS + h],
            {"sp": pair},
        )

    def to_place(role, to, h):
        return remote(
            to_peer.at[to * PARTS + h],
            from_peer.at[h],
            peer_send.at[role * PARTS + h],
            peer_recv.at[h],
            {"sp": to},
        )

    def to_pair(h):
        return remote(
            to_peer.at[pair * PARTS + h],
            from_peer.at[PARTS + h],
            peer_send.at[2 * PARTS + h],
            peer_recv.at[PARTS + h],
            {"sp": pair},
        )

    def compute(step, carry):
        turn = step // PARTS
        h = lax.rem(step, PARTS)
        role = jnp.where((turn == 3) | outer, turn, lax.rem(turn + 2, 3))
        to = jnp.where(role == 0, far, jnp.where(role == 1, near, jnp.where(role == 2, pair, z)))
        slot = to * PARTS + h
        rows = block(slot, part_rows)
        query_pos = slot * part_rows + lax.broadcasted_iota(jnp.int32, (part_rows, length), 0)
        key_pos = lax.broadcasted_iota(jnp.int32, (part_rows, length), 1)
        seen = query_pos >= key_pos
        mapped = []
        for m in range(2):
            part = slice(m * HEAD_DIM, (m + 1) * HEAD_DIM)
            scores = lax.dot_general(
                queries[rows, part],
                keys[:, part],
                (((1,), (1,)), ((), ())),
                preferred_element_type=jnp.float32,
            ) * HEAD_DIM ** (-0.5)
            scores = jnp.where(seen, scores, -jnp.inf)
            expons = jnp.exp(scores - jnp.max(scores, -1, keepdims=True))
            totals = jnp.sum(expons, -1, keepdims=True)
            mapped.append(
                jnp.dot(
                    expons.astype(jnp.bfloat16), values[...], preferred_element_type=jnp.float32
                )
                / totals
            )
        raw = mapped[0] - head_lambda * mapped[1]
        attn = (
            raw
            * lax.rsqrt(jnp.mean(raw * raw, -1, keepdims=True) + HEAD_EPS)
            * gain_ref[...]
            * HEAD_SCALE
        ).astype(jnp.bfloat16)
        extended = pools[
            pl.ds(pl.multiple_of(slot * part_rows, 16), part_rows + 16), :
        ].astype(jnp.float32)
        picked = extended + pltpu.roll(extended, 1, 0)
        sums = picked
        for shift in (2, 4, 8):
            sums = sums + pltpu.roll(sums, shift, 0)
            picked = lax.select_n(window >= 2 * shift, picked, sums)
        places_of = slot * part_rows + lax.broadcasted_iota(jnp.int32, (part_rows, 1), 0)
        counts = jnp.minimum(places_of + 1, window).astype(jnp.float32)
        mixed = (picked[16:] / counts - extended[16:]).astype(jnp.bfloat16)
        pooled = (
            jnp.dot(mixed, map_ref[z], preferred_element_type=jnp.float32) * scale_ref[z]
        ).astype(jnp.bfloat16)

        def partial_of(side):
            columns = block(side, half_out)
            return jnp.dot(
                pooled, outs[0, :, columns], preferred_element_type=jnp.float32
            ) + jnp.dot(attn, outs[1, :, columns], preferred_element_type=jnp.float32)

        to_mate[step] = partial_of(mate).astype(jnp.bfloat16)
        to_sibling(step).start()
        mine = partial_of(c)
        to_sibling(step).wait_recv()
        summed = mine + from_mate[step].astype(jnp.float32)

        @pl.when((role < 2) & outer)
        def _():
            to_peer[slot] = summed.astype(jnp.bfloat16)
            to_inner(role, to, h).start()

        @pl.when((role < 2) & jnp.logical_not(outer))
        def _():
            to_inner(role, to, h).wait_recv()
            to_peer[slot] = (
                summed + merging[role * PARTS + h].astype(jnp.float32)
            ).astype(jnp.bfloat16)
            to_place(role, to, h).start()

        @pl.when(role == 2)
        def _():
            to_peer[slot] = summed.astype(jnp.bfloat16)
            to_pair(h).start()

        @pl.when(role == 3)
        def _():
            final[h] = summed

        return carry

    lax.fori_loop(0, places * PARTS, compute, 0)

    for h in range(PARTS):
        to_pair(h).wait_recv()
        total = final[h] + from_peer[PARTS + h].astype(jnp.float32)
        to_place(0, z, h).wait_recv()
        out_ref[h * part_rows : (h + 1) * part_rows, :] = (
            total + from_peer[h].astype(jnp.float32)
        ).astype(out_ref.dtype)

    inward.drain()
    outward.drain()

    for p in range(PIECES):

        @pl.when(z < places - 1)
        def _():
            right(0, p).wait_send()

        @pl.when(z > 0)
        def _():
            left(0, p).wait_send()

        share(0, z, c, p).wait_send()
        for k in range(1, places):

            @pl.when(z >= k)
            def _():
                @pl.when(z < places - 1)
                def _():
                    right(k, p).wait_send()

                share(k, z - k, c, p).wait_send()

            @pl.when(z + k < places)
            def _():
                @pl.when(z > 0)
                def _():
                    left(k, p).wait_send()

                share(places - 1 + k, z + k, c, p).wait_send()

    for step in range(places * PARTS):
        to_sibling(step).wait_send()
    for h in range(PARTS):
        for role, to in ((0, far), (1, near)):

            @pl.when(outer)
            def _():
                to_inner(role, to, h).wait_send()

            @pl.when(jnp.logical_not(outer))
            def _():
                to_place(role, to, h).wait_send()

        to_pair(h).wait_send()


def fused(
    tokens,
    norm_gain,
    pool_input,
    query_weight,
    key_weight,
    value_weight,
    pool_map,
    pool_scale,
    head_gain,
    diff_lambda,
    out_pool,
    out_heads,
):
    places = lax.axis_size("sp")
    groups = lax.axis_size("fs")
    row_count, model = tokens.shape[1], tokens.shape[2]
    length = places * row_count
    half = HEAD_DIM // 2
    freqs = 1.0 / THETA ** (jnp.arange(half, dtype=jnp.float32) * 2.0 / HEAD_DIM)
    freqs = jnp.concatenate([freqs, freqs])[None, :]
    group_count = pool_map.shape[0]
    half_out = model // 2
    vmem = pl.BlockSpec(memory_space=pltpu.VMEM)
    smem = pl.BlockSpec(memory_space=pltpu.SMEM)
    dma = pltpu.SemaphoreType.DMA
    low = jnp.bfloat16

    def gather_sems(count):
        return [
            dma((count,)),
            dma((places, count)),
            dma((places, count)),
            dma((2, 2 * places)),
            dma((2, 2 * places)),
            dma((2, places)),
            dma((2, places)),
        ]

    out = pl.pallas_call(
        lambda *refs: fused_kernel(places, groups, *refs),
        out_shape=jax.ShapeDtypeStruct((row_count, half_out), low),
        in_specs=[vmem] * 10 + [smem] + [vmem] * 2,
        out_specs=vmem,
        scratch_shapes=[
            pltpu.VMEM((row_count // 2, model), low),
            pltpu.VMEM((length, HEAD_DIM), jnp.float32),
            pltpu.VMEM((length, HEAD_DIM), jnp.float32),
            pltpu.VMEM((length, model), low),
            pltpu.VMEM((4, model, GROUP_DIM), low),
            pltpu.VMEM((2, GROUP_DIM, model), low),
            pltpu.VMEM((length, GROUP_DIM), low),
            pltpu.VMEM((length, GROUP_DIM), low),
            pltpu.VMEM((length, GROUP_DIM), low),
            pltpu.VMEM((length + 16, GROUP_DIM), low),
            pltpu.VMEM((places * PARTS, row_count // PARTS, half_out), low),
            pltpu.VMEM((places * PARTS, row_count // PARTS, half_out), low),
            pltpu.VMEM((places * PARTS, row_count // PARTS, half_out), low),
            pltpu.VMEM((2 * PARTS, row_count // PARTS, half_out), low),
            pltpu.VMEM((2 * PARTS, row_count // PARTS, half_out), low),
            pltpu.VMEM((PARTS, row_count // PARTS, half_out), jnp.float32),
            dma,
            *gather_sems(4),
            *gather_sems(2),
            dma((places, PIECES)),
            dma((places + 1, PIECES)),
            dma((places, PIECES)),
            dma((places + 1, PIECES)),
            dma((2 * places, PIECES)),
            dma((2 * places, PIECES)),
            dma((places * PARTS,)),
            dma((places * PARTS,)),
            dma((3 * PARTS,)),
            dma((2 * PARTS,)),
            dma((2 * PARTS,)),
            dma((2 * PARTS,)),
        ],
        compiler_params=pltpu.CompilerParams(
            collective_id=0, has_side_effects=True, vmem_limit_bytes=56 * 1024 * 1024
        ),
    )(
        tokens[0],
        norm_gain.reshape(1, model),
        freqs,
        pool_input,
        query_weight,
        key_weight,
        value_weight,
        pool_map,
        pool_scale.reshape(group_count, 1, GROUP_DIM),
        head_gain.reshape(1, 2 * HEAD_DIM),
        diff_lambda,
        out_pool,
        out_heads,
    )
    return out[None]


def solution(mesh):
    placed = (
        P("fs", "sp", None),
        P(),
        P(("sp", "fs"), "tp"),
        P(("sp", "fs"), "tp"),
        P(("sp", "fs"), "tp"),
        P(("sp", "fs"), "tp"),
        P("tp", None, None),
        P("tp"),
        P(),
        P(),
        P("tp", ("sp", "fs")),
        P("tp", ("sp", "fs")),
    )
    shape = dict(mesh.shape)

    def body(tokens, *rest):
        head_count = rest[3].shape[1] // (2 * HEAD_DIM)
        group_count = rest[5].shape[0]
        fits = (
            shape["fs"] == 4
            and shape["tp"] == 2
            and shape["sp"] == head_count == group_count == 4
            and tokens.shape[0] == 1
        )
        return (fused if fits else local)(tokens, *rest)

    return jax.shard_map(
        body, mesh=mesh, in_specs=placed, out_specs=P("fs", "sp", "tp"), check_vma=False
    )
```

```python
import math

import jax
import jax.numpy as jnp
from jax import lax
from jax.experimental import pallas as pl
from jax.experimental.pallas import tpu as pltpu
from jax.sharding import PartitionSpec as P

HEAD_DIM = 128
GROUP_DIM = 256


THETA = 500000.0
HEAD_SCALE = 0.8
NORM_EPS = 1e-06
HEAD_EPS = 1e-05


def from_behind(value, axis, steps):
    count = lax.axis_size(axis)
    first, last = (max(0, -steps), min(count, count - steps))
    return lax.ppermute(value, axis, [(source, source + steps) for source in range(first, last)])


def rotate(tensor, positions):
    half = HEAD_DIM // 2
    freqs = 1.0 / THETA ** (jnp.arange(half, dtype=jnp.float32) * 2.0 / HEAD_DIM)
    angles = positions[:, None] * freqs[None, :]
    cosine = jnp.cos(angles)[:, None, None, :]
    sine = jnp.sin(angles)[:, None, None, :]
    floated = tensor.astype(jnp.float32)
    first = floated[..., :half]
    second = floated[..., half:]
    turned = jnp.concatenate([first * cosine - second * sine, second * cosine + first * sine], -1)
    return turned.astype(jnp.bfloat16)


def local(
    tokens,
    norm_gain,
    pool_input,
    query_weight,
    key_weight,
    value_weight,
    pool_map,
    pool_scale,
    head_gain,
    diff_lambda,
    out_pool,
    out_heads,
):
    out_local = jnp.concatenate([out_pool, out_heads], 0)
    row_count = tokens.shape[1]
    floated = tokens[0].astype(jnp.float32)
    normed = (
        floated * lax.rsqrt(jnp.mean(floated * floated, -1, keepdims=True) + NORM_EPS) * norm_gain
    ).astype(jnp.bfloat16)
    fragments = (
        lax.all_gather(pool_input, ("sp", "fs"), axis=0, tiled=True),
        lax.all_gather(query_weight, ("sp", "fs"), axis=0, tiled=True),
        lax.all_gather(key_weight, ("sp", "fs"), axis=0, tiled=True),
        lax.all_gather(value_weight, ("sp", "fs"), axis=0, tiled=True),
    )
    projected = tuple(
        (jnp.dot(normed, fragment, preferred_element_type=jnp.float32) for fragment in fragments)
    )
    pool_in, queries, keys_flat, values_flat = [
        product.astype(jnp.bfloat16) for product in projected
    ]
    head_count = values_flat.shape[1] // (2 * HEAD_DIM)
    tp_index = lax.axis_index("tp")
    sp_index = lax.axis_index("sp")
    query_pos = sp_index * row_count + jnp.arange(row_count, dtype=jnp.int32)
    positions = query_pos.astype(jnp.float32)
    queries = rotate(queries.reshape(row_count, head_count, 2, HEAD_DIM), positions)
    keys_flat = rotate(keys_flat.reshape(row_count, head_count, 2, HEAD_DIM), positions).reshape(
        row_count, head_count * 2 * HEAD_DIM
    )
    lambdas = lax.dynamic_slice_in_dim(diff_lambda, tp_index * head_count, head_count, 0)

    def online_step(state, key_rows, value_rows, key_offset):
        largest, summed, accum = state
        width = key_rows.shape[0]
        shaped = key_rows.reshape(width, head_count, 2, HEAD_DIM)
        scores = jnp.einsum(
            "qhcd,khcd->chqk", queries, shaped, preferred_element_type=jnp.float32
        ) * HEAD_DIM ** (-0.5)
        key_pos = key_offset + jnp.arange(width, dtype=jnp.int32)
        scores = jnp.where(query_pos[:, None] >= key_pos[None, :], scores, -jnp.inf)
        newest = jnp.maximum(largest, jnp.max(scores, -1))
        anchor = jnp.where(jnp.isfinite(newest), newest, 0.0)
        rescale = jnp.exp(largest - anchor)
        expons = jnp.exp(scores - anchor[..., None])
        summed = summed * rescale + jnp.sum(expons, -1)
        value_shaped = value_rows.reshape(width, head_count, 2 * HEAD_DIM)
        added = jnp.einsum(
            "chqk,khe->chqe",
            expons.astype(jnp.bfloat16),
            value_shaped,
            preferred_element_type=jnp.float32,
        )
        accum = accum * rescale[..., None] + added
        return (newest, summed, accum)

    start_state = (
        jnp.full((2, head_count, row_count), -jnp.inf, jnp.float32),
        jnp.zeros((2, head_count, row_count), jnp.float32),
        jnp.zeros((2, head_count, row_count, 2 * HEAD_DIM), jnp.float32),
    )
    fragments = (
        lax.all_gather(keys_flat, "sp", axis=0, tiled=True),
        lax.all_gather(values_flat, "sp", axis=0, tiled=True),
    )
    span = math.gcd(fragments[0].shape[0], 1024)

    def inner_step(index, inner_state):
        key_rows = lax.dynamic_slice_in_dim(fragments[0], index * span, span, 0)
        value_rows = lax.dynamic_slice_in_dim(fragments[1], index * span, span, 0)
        return online_step(inner_state, key_rows, value_rows, index * span)

    final_state = lax.fori_loop(0, fragments[0].shape[0] // span, inner_step, start_state)
    summed_final = final_state[1]
    accum_final = final_state[2]
    heads_raw = (
        accum_final[0] / summed_final[0][..., None]
        - lambdas[:, None, None] * accum_final[1] / summed_final[1][..., None]
    )
    heads_raw = jnp.moveaxis(heads_raw, 0, 1)
    attn = (
        (
            heads_raw
            * lax.rsqrt(jnp.mean(heads_raw * heads_raw, -1, keepdims=True) + HEAD_EPS)
            * head_gain
            * HEAD_SCALE
        )
        .astype(jnp.bfloat16)
        .reshape(row_count, head_count * 2 * HEAD_DIM)
    )
    reach = 15
    rim_rows = from_behind(pool_in[row_count - reach :], "sp", 1)
    extended = jnp.concatenate([rim_rows, pool_in], 0).astype(jnp.float32)
    pair_sums = extended[1:] + extended[:-1]
    quad_sums = pair_sums[2:] + pair_sums[:-2]
    octet_sums = quad_sums[4:] + quad_sums[:-4]
    sixteen_sums = octet_sums[8:] + octet_sums[:-8]
    group_count = pool_in.shape[1] // GROUP_DIM
    stacked = jnp.stack(
        [
            pair_sums[14 : 14 + row_count],
            quad_sums[12 : 12 + row_count],
            octet_sums[8 : 8 + row_count],
            sixteen_sums,
        ],
        0,
    ).reshape(4, row_count, group_count, GROUP_DIM)
    levels = (tp_index * group_count + jnp.arange(group_count, dtype=jnp.int32)) % 4
    picked = jnp.sum(
        jnp.where(
            levels[None, None, :, None] == jnp.arange(4, dtype=jnp.int32)[:, None, None, None],
            stacked,
            0.0,
        ),
        0,
    )
    windows = 2 ** (1 + levels)
    counts = jnp.minimum(query_pos[:, None] + 1, windows[None, :]).astype(jnp.float32)
    window_mean = picked / counts[:, :, None]
    grouped = pool_in.reshape(row_count, group_count, GROUP_DIM).astype(jnp.float32)
    pool_mixed = (window_mean - grouped).astype(jnp.bfloat16)
    pooled = (
        (
            jnp.einsum("tgc,gce->tge", pool_mixed, pool_map, preferred_element_type=jnp.float32)
            * pool_scale.reshape(group_count, GROUP_DIM)
        )
        .astype(jnp.bfloat16)
        .reshape(row_count, group_count * GROUP_DIM)
    )
    branches = jnp.concatenate([pooled, attn], 1)
    partial_value = jnp.dot(
        branches,
        lax.all_gather(out_local, ("sp", "fs"), axis=1, tiled=True),
        preferred_element_type=jnp.float32,
    )
    layer_out = lax.psum_scatter(
        partial_value.astype(jnp.bfloat16), "tp", scatter_dimension=1, tiled=True
    )
    return layer_out[None]


MESH = pl.DeviceIdType.MESH
PIECES = 4
PARTS = 2

def fused_kernel(
    places,
    groups,
    tokens_ref,
    norm_gain_ref,
    freqs_ref,
    pool_ref,
    query_ref,
    key_ref,
    value_ref,
    map_ref,
    scale_ref,
    gain_ref,
    lambda_ref,
    out_pool_ref,
    out_heads_ref,
    out_ref,
    normed_ref,
    cos_ref,
    sin_ref,
    rows_all,
    weights,
    outs,
    queries,
    keys,
    values,
    pools,
    to_mate,
    from_mate,
    to_peer,
    from_peer,
    merging,
    final,
    pooled_all,
    attn_all,
    *sems,
):
    (
        own_sem,
        in_local,
        in_z_send,
        in_z_recv,
        in_n_send,
        in_n_recv,
        in_f_send,
        in_f_recv,
        out_local,
        out_z_send,
        out_z_recv,
        out_n_send,
        out_n_recv,
        out_f_send,
        out_f_recv,
        right_send,
        right_recv,
        left_send,
        left_recv,
        mate_send,
        mate_recv,
        half_send,
        half_recv,
        peer_send,
        peer_recv,
        merge_send,
        merge_recv,
    ) = sems
    z = lax.axis_index("sp")
    f = lax.axis_index("fs")
    c = lax.axis_index("tp")
    fx = f + 1 - 2 * lax.rem(f, 2)
    fy = lax.rem(f + 2, groups)
    mate = 1 - c
    half_rows = tokens_ref.shape[0] // 2
    row_count = 2 * half_rows
    depth = pool_ref.shape[0]
    width = GROUP_DIM
    out_width = out_pool_ref.shape[1]
    half_out = out_ref.shape[1]

    barrier = pltpu.get_barrier_semaphore()
    partners = [{"sp": lax.rem(z + d, places)} for d in range(1, places)]
    partners += [{"fs": fx}, {"fs": fy}, {"tp": mate}]
    for partner in partners:
        pl.semaphore_signal(barrier, inc=1, device_id=partner, device_id_type=MESH)
    pl.semaphore_wait(barrier, len(partners))

    def remote(source, target, send, recv, device):
        return pltpu.make_async_remote_copy(
            src_ref=source,
            dst_ref=target,
            send_sem=send,
            recv_sem=recv,
            device_id=device,
            device_id_type=MESH,
        )

    def block(index, size):
        return pl.ds(pl.multiple_of(index * size, size), size)

    class Gather:
        def __init__(self, sources, cut, view, group):
            self.sources, self.cut, self.view = sources, cut, view
            self.count = len(sources)
            (
                self.local,
                self.z_send,
                self.z_recv,
                self.n_send,
                self.n_recv,
                self.f_send,
                self.f_recv,
            ) = group
            self.low = (0, self.count // 2)
            self.high = (self.count // 2, self.count - self.count // 2)

        def own(self, m):
            return pltpu.make_async_copy(
                self.cut(self.sources[m], z), self.view(z, f, m, 1).at[0], self.local.at[m]
            )

        def across(self, d, m):
            to = lax.rem(z + d, places)
            return remote(
                self.cut(self.sources[m], to),
                self.view(z, f, m, 1).at[0],
                self.z_send.at[d, m],
                self.z_recv.at[d, m],
                {"sp": to},
            )

        def arrive(self, d, m):
            view = self.view(lax.rem(z + places - d, places), f, m, 1).at[0]
            return remote(
                view,
                view,
                self.z_send.at[d, m],
                self.z_recv.at[d, m],
                {"sp": lax.rem(z + places - d, places)},
            )

        def near(self, d, side, column, half):
            start, size = (self.low, self.high)[half]
            view = self.view(lax.rem(z + places - d, places), column, start, size)
            return remote(
                view,
                view,
                self.n_send.at[side, 2 * d + half],
                self.n_recv.at[side, 2 * d + half],
                {"fs": (fx, fy)[side]},
            )

        def forward(self, d, side, column):
            start, size = (self.high, self.low)[side]
            view = self.view(lax.rem(z + places - d, places), column, start, size)
            return remote(
                view,
                view,
                self.f_send.at[side, d],
                self.f_recv.at[side, d],
                {"fs": (fx, fy)[side]},
            )

        def start_own(self):
            for m in range(self.count):
                self.own(m).start()

        def start(self):
            for d in range(1, places):
                for m in range(self.count):
                    self.across(d, m).start()

        def first(self, d):
            for m in range(self.count):
                if isinstance(d, int) and d == 0:
                    self.own(m).wait()
                else:
                    self.arrive(d, m).wait_recv()
            for order in range(2):
                for side in range(2):
                    self.near(d, side, f, side ^ order).start()

        def second(self, d):
            self.near(d, 0, fx, 0).wait_recv()
            self.forward(d, 1, fx).start()
            self.near(d, 1, fy, 1).wait_recv()
            self.forward(d, 0, fy).start()

        def third(self, d):
            diagonal = lax.rem(fx + 2, groups)
            for side in range(2):
                self.forward(d, side, diagonal).wait_recv()
            self.near(d, 0, fx, 1).wait_recv()
            self.near(d, 1, fy, 0).wait_recv()

        def drain(self):
            for d in range(places):
                for m in range(self.count):
                    if d > 0:
                        self.across(d, m).wait_send()
                for side in range(2):
                    for half in range(2):
                        self.near(d, side, f, half).wait_send()
                self.forward(d, 1, fx).wait_send()
                self.forward(d, 0, fy).wait_send()

    inward = Gather(
        (pool_ref, query_ref, key_ref, value_ref),
        lambda ref, to: ref.at[:, block(to, width)],
        lambda zz, ff, m, n: weights.at[pl.ds(m, n), block(zz * groups + ff, depth), :],
        (in_local, in_z_send, in_z_recv, in_n_send, in_n_recv, in_f_send, in_f_recv),
    )
    outward = Gather(
        (out_pool_ref, out_heads_ref),
        lambda ref, to: ref.at[block(to, width), :],
        lambda zz, ff, m, n: outs.at[pl.ds(m, n), :, block(zz * groups + ff, out_width)],
        (out_local, out_z_send, out_z_recv, out_n_send, out_n_recv, out_f_send, out_f_recv),
    )

    piece_rows = half_rows // PIECES

    def chunk(zz, side, p):
        return rows_all.at[block((2 * zz + side) * PIECES + p, piece_rows), :]

    def right(k, p):
        view = chunk(z - k, c, p)
        return remote(view, view, right_send.at[k, p], right_recv.at[k + 1, p], {"sp": z + 1})

    def from_left(k, p):
        view = chunk(z - k, c, p)
        return remote(view, view, right_send.at[k, p], right_recv.at[k, p], {"sp": z - 1})

    def left(k, p):
        view = chunk(z + k, c, p)
        return remote(view, view, left_send.at[k, p], left_recv.at[k + 1, p], {"sp": z - 1})

    def from_right(k, p):
        view = chunk(z + k, c, p)
        return remote(view, view, left_send.at[k, p], left_recv.at[k, p], {"sp": z + 1})

    def share(slot, zz, side, p):
        view = chunk(zz, side, p)
        return remote(view, view, mate_send.at[slot, p], mate_recv.at[slot, p], {"tp": mate})

    own_rows = pltpu.make_async_copy(
        normed_ref, rows_all.at[block(2 * z + c, half_rows), :], own_sem
    )
    inward.start_own()
    inward.start()
    outward.start_own()
    floated = tokens_ref[pl.ds(pl.multiple_of(c * half_rows, 16), half_rows), :].astype(
        jnp.float32
    )
    normed_ref[...] = (
        floated
        * lax.rsqrt(jnp.mean(floated * floated, -1, keepdims=True) + NORM_EPS)
        * norm_gain_ref[...]
    ).astype(jnp.bfloat16)
    own_rows.start()
    own_rows.wait()

    @pl.when(z < places - 1)
    def _():
        for p in range(PIECES):
            right(0, p).start()

    @pl.when(z > 0)
    def _():
        for p in range(PIECES):
            left(0, p).start()

    for p in range(PIECES):
        share(0, z, c, p).start()

    def tokens_step(k):
        for p in range(PIECES):

            @pl.when(z >= k)
            def _():
                from_left(k, p).wait_recv()

                @pl.when(z < places - 1)
                def _():
                    right(k, p).start()

                share(k, z - k, c, p).start()

            @pl.when(z + k < places)
            def _():
                from_right(k, p).wait_recv()

                @pl.when(z > 0)
                def _():
                    left(k, p).start()

                share(places - 1 + k, z + k, c, p).start()

    pools[0:16, :] = jnp.zeros((16, width), jnp.bfloat16)
    inward.first(0)

    def table(index, carry):
        rows = block(index, row_count)
        half = HEAD_DIM // 2
        count = (
            index * row_count + lax.broadcasted_iota(jnp.int32, (row_count, HEAD_DIM), 0)
        ).astype(jnp.float32)
        lane = lax.broadcasted_iota(jnp.int32, (row_count, HEAD_DIM), 1)
        angles = count * freqs_ref[...]
        cos_ref[rows, :] = jnp.cos(angles)
        sine = jnp.sin(angles)
        sin_ref[rows, :] = jnp.where(lane < half, -sine, sine)
        return carry

    lax.fori_loop(0, places, table, 0)
    for d in range(1, places):
        inward.first(d)
        inward.second(d - 1)
    outward.first(0)
    inward.second(places - 1)
    for k in range(1, places - 1):
        tokens_step(k)
    outward.start()
    outward.second(0)
    tokens_step(places - 1)
    for d in range(places):
        inward.third(d)

    for p in range(PIECES):
        share(0, z, mate, p).wait_recv()
        for k in range(1, places):

            @pl.when(z >= k)
            def _():
                share(k, z - k, mate, p).wait_recv()

            @pl.when(z + k < places)
            def _():
                share(places - 1 + k, z + k, mate, p).wait_recv()

    def turned(raw, cosine, sine):
        floated = raw.astype(jnp.float32)
        return (floated * cosine + pltpu.roll(floated, HEAD_DIM // 2, 1) * sine).astype(
            jnp.bfloat16
        )

    def project(index, carry):
        rows = block(index, row_count)
        normed = rows_all[rows, :]
        cosine = cos_ref[rows, :]
        sine = sin_ref[rows, :]

        def product(m):
            return jnp.dot(normed, weights[m], preferred_element_type=jnp.float32).astype(
                jnp.bfloat16
            )

        pools[pl.ds(pl.multiple_of(index * row_count + 16, 16), row_count), :] = product(0)
        raw = product(1)
        for m in range(2):
            part = slice(m * HEAD_DIM, (m + 1) * HEAD_DIM)
            queries[rows, part] = turned(raw[:, part], cosine, sine)
        raw = product(2)
        for m in range(2):
            part = slice(m * HEAD_DIM, (m + 1) * HEAD_DIM)
            keys[rows, part] = turned(raw[:, part], cosine, sine)
        values[rows, :] = product(3)
        return carry

    lax.fori_loop(0, places, project, 0)

    level = lax.rem(c * map_ref.shape[0] + z, 4)
    window = jnp.where(
        level == 0, 2, jnp.where(level == 1, 4, jnp.where(level == 2, 8, 16))
    )
    head_lambda = lambda_ref[c * map_ref.shape[0] + z]
    length = places * row_count

    def attend(index, carry):
        rows = block(index, row_count)
        query_pos = index * row_count + lax.broadcasted_iota(jnp.int32, (row_count, length), 0)
        key_pos = lax.broadcasted_iota(jnp.int32, (row_count, length), 1)
        seen = query_pos >= key_pos
        mapped = []
        for m in range(2):
            part = slice(m * HEAD_DIM, (m + 1) * HEAD_DIM)
            scores = lax.dot_general(
                queries[rows, part],
                keys[:, part],
                (((1,), (1,)), ((), ())),
                preferred_element_type=jnp.float32,
            ) * HEAD_DIM ** (-0.5)
            scores = jnp.where(seen, scores, -jnp.inf)
            expons = jnp.exp(scores - jnp.max(scores, -1, keepdims=True))
            totals = jnp.sum(expons, -1, keepdims=True)
            mapped.append(
                jnp.dot(
                    expons.astype(jnp.bfloat16), values[...], preferred_element_type=jnp.float32
                )
                / totals
            )
        raw = mapped[0] - head_lambda * mapped[1]
        attn = (
            raw
            * lax.rsqrt(jnp.mean(raw * raw, -1, keepdims=True) + HEAD_EPS)
            * gain_ref[...]
            * HEAD_SCALE
        ).astype(jnp.bfloat16)
        extended = pools[
            pl.ds(pl.multiple_of(index * row_count, 16), row_count + 16), :
        ].astype(jnp.float32)
        picked = extended + pltpu.roll(extended, 1, 0)
        sums = picked
        for shift in (2, 4, 8):
            sums = sums + pltpu.roll(sums, shift, 0)
            picked = lax.select_n(window >= 2 * shift, picked, sums)
        places_of = index * row_count + lax.broadcasted_iota(jnp.int32, (row_count, 1), 0)
        counts = jnp.minimum(places_of + 1, window).astype(jnp.float32)
        mixed = (picked[16:] / counts - extended[16:]).astype(jnp.bfloat16)
        pooled = (
            jnp.dot(mixed, map_ref[z], preferred_element_type=jnp.float32) * scale_ref[z]
        ).astype(jnp.bfloat16)
        pooled_all[rows, :] = pooled
        attn_all[rows, :] = attn

        @pl.when(index < places - 1)
        def _():
            outward.first(index + 1)

        @pl.when((index > 0) & (index < places - 1))
        def _():
            outward.second(index)

        return carry

    lax.fori_loop(0, places, attend, 0)
    outward.second(places - 1)
    for d in range(places):
        outward.third(d)

    part_rows = row_count // PARTS

    def to_sibling(step):
        return remote(
            to_mate.at[step],
            from_mate.at[step],
            half_send.at[step],
            half_recv.at[step],
            {"tp": mate},
        )

    outer = (z == 0) | (z == places - 1)
    pair = z + 1 - 2 * lax.rem(z, 2)
    far = jnp.where(z < 2, places - 1, 0)
    near = jnp.where(z < 2, 2, 1)

    def to_inner(role, to, h):
        return remote(
            to_peer.at[to * PARTS + h],
            merging.at[role * PARTS + h],
            merge_send.at[role * PARTS + h],
            merge_recv.at[role * PARTS + h],
            {"sp": pair},
        )

    def to_place(role, to, h):
        return remote(
            to_peer.at[to * PARTS + h],
            from_peer.at[h],
            peer_send.at[role * PARTS + h],
            peer_recv.at[h],
            {"sp": to},
        )

    def to_pair(h):
        return remote(
            to_peer.at[pair * PARTS + h],
            from_peer.at[PARTS + h],
            peer_send.at[2 * PARTS + h],
            peer_recv.at[PARTS + h],
            {"sp": pair},
        )

    def compute(step, carry):
        turn = step // PARTS
        h = lax.rem(step, PARTS)
        role = jnp.where((turn == 3) | outer, turn, lax.rem(turn + 2, 3))
        to = jnp.where(role == 0, far, jnp.where(role == 1, near, jnp.where(role == 2, pair, z)))
        slot = to * PARTS + h
        rows = block(slot, part_rows)
        pooled = pooled_all[rows, :]
        attn = attn_all[rows, :]

        def partial_of(side):
            columns = block(side, half_out)
            return jnp.dot(
                pooled, outs[0, :, columns], preferred_element_type=jnp.float32
            ) + jnp.dot(attn, outs[1, :, columns], preferred_element_type=jnp.float32)

        to_mate[step] = partial_of(mate).astype(jnp.bfloat16)
        to_sibling(step).start()
        mine = partial_of(c)
        to_sibling(step).wait_recv()
        summed = mine + from_mate[step].astype(jnp.float32)

        @pl.when((role < 2) & outer)
        def _():
            to_peer[slot] = summed.astype(jnp.bfloat16)
            to_inner(role, to, h).start()

        @pl.when((role < 2) & jnp.logical_not(outer))
        def _():
            to_inner(role, to, h).wait_recv()
            to_peer[slot] = (
                summed + merging[role * PARTS + h].astype(jnp.float32)
            ).astype(jnp.bfloat16)
            to_place(role, to, h).start()

        @pl.when(role == 2)
        def _():
            to_peer[slot] = summed.astype(jnp.bfloat16)
            to_pair(h).start()

        @pl.when(role == 3)
        def _():
            final[h] = summed

        return carry

    lax.fori_loop(0, places * PARTS, compute, 0)

    for h in range(PARTS):
        to_pair(h).wait_recv()
        total = final[h] + from_peer[PARTS + h].astype(jnp.float32)
        to_place(0, z, h).wait_recv()
        out_ref[h * part_rows : (h + 1) * part_rows, :] = (
            total + from_peer[h].astype(jnp.float32)
        ).astype(out_ref.dtype)

    inward.drain()
    outward.drain()

    for p in range(PIECES):

        @pl.when(z < places - 1)
        def _():
            right(0, p).wait_send()

        @pl.when(z > 0)
        def _():
            left(0, p).wait_send()

        share(0, z, c, p).wait_send()
        for k in range(1, places):

            @pl.when(z >= k)
            def _():
                @pl.when(z < places - 1)
                def _():
                    right(k, p).wait_send()

                share(k, z - k, c, p).wait_send()

            @pl.when(z + k < places)
            def _():
                @pl.when(z > 0)
                def _():
                    left(k, p).wait_send()

                share(places - 1 + k, z + k, c, p).wait_send()

    for step in range(places * PARTS):
        to_sibling(step).wait_send()
    for h in range(PARTS):
        for role, to in ((0, far), (1, near)):

            @pl.when(outer)
            def _():
                to_inner(role, to, h).wait_send()

            @pl.when(jnp.logical_not(outer))
            def _():
                to_place(role, to, h).wait_send()

        to_pair(h).wait_send()


def fused(
    tokens,
    norm_gain,
    pool_input,
    query_weight,
    key_weight,
    value_weight,
    pool_map,
    pool_scale,
    head_gain,
    diff_lambda,
    out_pool,
    out_heads,
):
    places = lax.axis_size("sp")
    groups = lax.axis_size("fs")
    row_count, model = tokens.shape[1], tokens.shape[2]
    length = places * row_count
    half = HEAD_DIM // 2
    freqs = 1.0 / THETA ** (jnp.arange(half, dtype=jnp.float32) * 2.0 / HEAD_DIM)
    freqs = jnp.concatenate([freqs, freqs])[None, :]
    group_count = pool_map.shape[0]
    half_out = model // 2
    vmem = pl.BlockSpec(memory_space=pltpu.VMEM)
    smem = pl.BlockSpec(memory_space=pltpu.SMEM)
    dma = pltpu.SemaphoreType.DMA
    low = jnp.bfloat16

    def gather_sems(count):
        return [
            dma((count,)),
            dma((places, count)),
            dma((places, count)),
            dma((2, 2 * places)),
            dma((2, 2 * places)),
            dma((2, places)),
            dma((2, places)),
        ]

    out = pl.pallas_call(
        lambda *refs: fused_kernel(places, groups, *refs),
        out_shape=jax.ShapeDtypeStruct((row_count, half_out), low),
        in_specs=[vmem] * 10 + [smem] + [vmem] * 2,
        out_specs=vmem,
        scratch_shapes=[
            pltpu.VMEM((row_count // 2, model), low),
            pltpu.VMEM((length, HEAD_DIM), jnp.float32),
            pltpu.VMEM((length, HEAD_DIM), jnp.float32),
            pltpu.VMEM((length, model), low),
            pltpu.VMEM((4, model, GROUP_DIM), low),
            pltpu.VMEM((2, GROUP_DIM, model), low),
            pltpu.VMEM((length, GROUP_DIM), low),
            pltpu.VMEM((length, GROUP_DIM), low),
            pltpu.VMEM((length, GROUP_DIM), low),
            pltpu.VMEM((length + 16, GROUP_DIM), low),
            pltpu.VMEM((places * PARTS, row_count // PARTS, half_out), low),
            pltpu.VMEM((places * PARTS, row_count // PARTS, half_out), low),
            pltpu.VMEM((places * PARTS, row_count // PARTS, half_out), low),
            pltpu.VMEM((2 * PARTS, row_count // PARTS, half_out), low),
            pltpu.VMEM((2 * PARTS, row_count // PARTS, half_out), low),
            pltpu.VMEM((PARTS, row_count // PARTS, half_out), jnp.float32),
            pltpu.VMEM((length, GROUP_DIM), low),
            pltpu.VMEM((length, GROUP_DIM), low),
            dma,
            *gather_sems(4),
            *gather_sems(2),
            dma((places, PIECES)),
            dma((places + 1, PIECES)),
            dma((places, PIECES)),
            dma((places + 1, PIECES)),
            dma((2 * places, PIECES)),
            dma((2 * places, PIECES)),
            dma((places * PARTS,)),
            dma((places * PARTS,)),
            dma((3 * PARTS,)),
            dma((2 * PARTS,)),
            dma((2 * PARTS,)),
            dma((2 * PARTS,)),
        ],
        compiler_params=pltpu.CompilerParams(
            collective_id=0, has_side_effects=True, vmem_limit_bytes=56 * 1024 * 1024
        ),
    )(
        tokens[0],
        norm_gain.reshape(1, model),
        freqs,
        pool_input,
        query_weight,
        key_weight,
        value_weight,
        pool_map,
        pool_scale.reshape(group_count, 1, GROUP_DIM),
        head_gain.reshape(1, 2 * HEAD_DIM),
        diff_lambda,
        out_pool,
        out_heads,
    )
    return out[None]


def solution(mesh):
    placed = (
        P("fs", "sp", None),
        P(),
        P(("sp", "fs"), "tp"),
        P(("sp", "fs"), "tp"),
        P(("sp", "fs"), "tp"),
        P(("sp", "fs"), "tp"),
        P("tp", None, None),
        P("tp"),
        P(),
        P(),
        P("tp", ("sp", "fs")),
        P("tp", ("sp", "fs")),
    )
    shape = dict(mesh.shape)

    def body(tokens, *rest):
        head_count = rest[3].shape[1] // (2 * HEAD_DIM)
        group_count = rest[5].shape[0]
        fits = (
            shape["fs"] == 4
            and shape["tp"] == 2
            and shape["sp"] == head_count == group_count == 4
            and tokens.shape[0] == 1
        )
        return (fused if fits else local)(tokens, *rest)

    return jax.shard_map(
        body, mesh=mesh, in_specs=placed, out_specs=P("fs", "sp", "tp"), check_vma=False
    )
```
